256 devices in a mesh: sp: 32 (over z, y), tp: 8 (over x, core).
Axes of the slice: x: 4, y: 4, z: 8, core: 2. Of those that a mesh axis runs over, the one named last changes fastest.
Arguments:
- queries: bfloat16 [16384, 1024], P('sp', 'tp'), may hold values from -200 to 200
- keys: bfloat16 [16384, 1024], P('sp', 'tp'), may hold values from -6 to 6
- values: bfloat16 [16384, 1024], P('sp', 'tp'), may hold values from -24 to 24
- cum_gate: float32 [16384, 8], P('sp', 'tp'), may hold values from -1643 to 0, as said below
- residual: bfloat16 [16384, 2048], P(('sp', 'tp')), may hold values from -1.5 to 1.5
- w_out: bfloat16 [1024, 2048], replicated, may hold values from -0.1875 to 0.1875
- gain: float32 [2048], replicated, may hold values from 0.1 to 1.9
- w_up: bfloat16 [2048, 8192], P('sp', 'tp'), may hold values from -0.125 to 0.125
- w_down: bfloat16 [8192, 2048], P('tp', 'sp'), may hold values from -0.0625 to 0.0625
Outputs:
- output: bfloat16 [16384, 2048], P(('sp', 'tp'))
The draws below stay inside these ranges and needn't reach their ends.
Inputs may be any that keep to these rules, and one draw needn't show every extreme that they name: Within each head, cum_gate never rises from one position to the next.
All inputs are finite; a program needn't handle non-finite values.
Results may differ from the reference program's by a relative error of at most 0.022.
Values may be sent and summed in bfloat16 or wider, within the bound.
A program may use at most 128 MiB of HBM per device.

```python
import math
import jax
import jax.numpy as jnp
from jax import lax

D = 2048
HEADS = 8
HEAD_DIM = 128
FF = 8192
TOK_DEV = 512
SEQUENCE_TOKENS = 16384
N_TP = 8


def joint_pair(key):
    width = HEADS * HEAD_DIM
    query_key = jax.random.fold_in(key, 101)
    key_key = jax.random.fold_in(key, 202)
    keys = jnp.clip(jax.random.normal(key_key, (SEQUENCE_TOKENS, width), jnp.float32), -6.0, 6.0)
    queries = jnp.clip(2.0 * jax.random.normal(query_key, (SEQUENCE_TOKENS, width), jnp.float32), -12.0, 12.0)
    return (queries, keys)


def draw_queries(key, part):
    return joint_pair(key)[0].astype(jnp.bfloat16)


def draw_keys(key, part):
    return joint_pair(key)[1].astype(jnp.bfloat16)


def draw_cum_gate(key, part):
    shuffle_random_key, gradual_decay_key, quick_decay_key, block_random_key, jitter_random_key, spike_random_key, layer_depth_key = jax.random.split(key, 7)
    order = jax.random.permutation(shuffle_random_key, HEADS)
    slow = order < HEADS // 2
    slow_rate = jax.random.uniform(gradual_decay_key, (HEADS,), jnp.float32, 0.2, 0.6) / SEQUENCE_TOKENS
    fast_rate = 1.0 / jnp.exp(jax.random.uniform(quick_decay_key, (HEADS,), jnp.float32, math.log(30.0), math.log(100.0)))
    rate = jnp.where(slow, slow_rate, fast_rate)
    shards = SEQUENCE_TOKENS // TOK_DEV
    factor = 2.0 ** jax.random.uniform(block_random_key, (shards, HEADS), jnp.float32, -1.0, 1.0)
    token_positions = jnp.arange(SEQUENCE_TOKENS)
    per_row = factor[token_positions // TOK_DEV]
    noise = jax.random.uniform(jitter_random_key, (SEQUENCE_TOKENS, HEADS), jnp.float32, 0.5, 1.5)
    steps = -rate[None, :] * per_row * noise
    spike_events = jax.random.randint(spike_random_key, (3,), 0, SEQUENCE_TOKENS)
    depth = jnp.log(jax.random.uniform(layer_depth_key, (3, HEADS), jnp.float32, 0.6, 0.8))
    match_events = (token_positions[:, None] == spike_events[None, :]).astype(jnp.float32)
    steps = steps + jnp.dot(match_events, depth) * slow.astype(jnp.float32)[None, :]
    return jnp.cumsum(steps, axis=0)


def level_of(own_key, extent, pieces, smallest, top_value):
    level, own = 1.0, jax.random.fold_in(own_key, 6)
    for axis_at, shards_of in pieces:
        heights = jnp.exp(jax.random.uniform(jax.random.fold_in(own, axis_at), (shards_of,), jnp.float32, smallest / len(pieces), top_value / len(pieces)))
        level = level * jnp.repeat(heights, extent[axis_at] // shards_of).reshape([-1 if axis == axis_at else 1 for axis in range(len(extent))])
    return level


def centred(rng, shape, scale, limit, pieces=(), held_as=jnp.bfloat16):
    drawn = jax.random.normal(rng, shape, jnp.float32) * scale
    if len(pieces) > 0:
        drawn = level_of(rng, shape, pieces, -0.22, 0.18) * drawn
    return jnp.clip(drawn, min=-limit, max=limit).astype(held_as)


def setup_inputs(seed: int = 0) -> dict:
    streams_of = jax.random.split(jax.random.key(seed), 10)
    queries = draw_queries(jax.random.fold_in(streams_of[9], 71), 0)
    keys = draw_keys(jax.random.fold_in(streams_of[9], 71), 0)
    values = centred(streams_of[2], (SEQUENCE_TOKENS, HEADS * HEAD_DIM), 4.0, 24.0, ((0, 32), (1, 8)))
    cum_gate = draw_cum_gate(jax.random.fold_in(streams_of[9], 71), 0)
    residual = centred(streams_of[4], (SEQUENCE_TOKENS, D), 0.25, 1.5, ((0, 256),))
    w_out = centred(streams_of[5], (HEADS * HEAD_DIM, D), (HEADS * HEAD_DIM) ** -0.5, 0.1875)
    gain = jnp.clip(1.0 + 0.18 * jax.random.normal(streams_of[6], (D,), jnp.float32), 0.1, 1.9)
    w_up = centred(streams_of[7], (D, FF), D ** -0.5, 0.125, ((0, 32), (1, 8)))
    w_down = centred(streams_of[8], (FF, D), FF ** -0.5, 0.0625, ((0, 8), (1, 32)))
    return dict(queries=queries, keys=keys, values=values, cum_gate=cum_gate, residual=residual, w_out=w_out, gain=gain, w_up=w_up, w_down=w_down)


def reference(queries, keys, values, cum_gate, residual, w_out, gain, w_up, w_down):
    width = HEADS * HEAD_DIM
    q_block = math.gcd(SEQUENCE_TOKENS, 512)
    key_heads = keys.astype(jnp.float32).reshape(SEQUENCE_TOKENS, HEADS, HEAD_DIM)
    value_heads = values.astype(jnp.float32).reshape(SEQUENCE_TOKENS, HEADS, HEAD_DIM)
    key_pos = jnp.arange(SEQUENCE_TOKENS, dtype=jnp.int32)
    gate_rows = cum_gate.T

    def attend(block_index):
        offset = (block_index * q_block).astype(jnp.int32)
        query_blk = lax.dynamic_slice_in_dim(queries, offset, q_block, 0).astype(jnp.float32)
        query_blk = query_blk.reshape(q_block, HEADS, HEAD_DIM)
        gate_blk = lax.dynamic_slice_in_dim(cum_gate, offset, q_block, 0)
        scores = jnp.einsum('qhd,khd->qhk', query_blk, key_heads) * HEAD_DIM ** (-0.5)
        scores = scores + gate_blk[:, :, None] - gate_rows[None, :, :]
        query_pos = offset + jnp.arange(q_block, dtype=jnp.int32)
        scores = jnp.where(key_pos[None, None, :] <= query_pos[:, None, None], scores, -1e+30)
        top = lax.optimization_barrier(jnp.max(scores, axis=-1, keepdims=True))
        weights = jnp.exp(scores - top)
        denom = lax.optimization_barrier(jnp.sum(weights, axis=-1))
        rounded = lax.optimization_barrier(weights.astype(jnp.bfloat16)).astype(jnp.float32)
        numer = jnp.einsum('qhk,khd->qhd', rounded, value_heads)
        return (numer / denom[:, :, None]).reshape(q_block, width).astype(jnp.bfloat16)
    blocks = lax.map(attend, jnp.arange(SEQUENCE_TOKENS // q_block, dtype=jnp.int32))
    attended = blocks.reshape(SEQUENCE_TOKENS, width)
    residual_sum = residual.astype(jnp.float32) + jnp.dot(attended, w_out, preferred_element_type=jnp.float32)
    mean_square = lax.optimization_barrier(jnp.mean(residual_sum * residual_sum, axis=-1, keepdims=True))
    normed = (residual_sum * lax.rsqrt(mean_square + 1e-06) * gain).astype(jnp.bfloat16)
    up_proj = jnp.dot(normed, w_up, preferred_element_type=jnp.float32)
    hidden = jnp.square(jax.nn.relu(up_proj)).astype(jnp.bfloat16)
    group = FF // N_TP
    summed = jnp.zeros((SEQUENCE_TOKENS, D), jnp.float32)
    for index in range(N_TP):
        part_out = jnp.dot(hidden[:, index * group:(index + 1) * group], w_down[index * group:(index + 1) * group], preferred_element_type=jnp.float32).astype(jnp.bfloat16)
        summed = summed + lax.optimization_barrier(part_out).astype(jnp.float32)
    return (residual_sum + summed).astype(jnp.bfloat16)
```

```python
import functools
import math

import jax
import jax.numpy as jnp
from jax import lax
from jax.experimental import pallas as pl
from jax.experimental.pallas import tpu as pltpu
from jax.sharding import Mesh
from jax.sharding import PartitionSpec as P

MESH = pl.DeviceIdType.MESH
GRID = (8, 4, 4, 2)
ROW_TILE = 256
COL_TILE = 256
GROUPS = 4
LOW = -1e30


def remote(src, dst, send_sem, recv_sem, device):
    return pltpu.make_async_remote_copy(
        src_ref=src,
        dst_ref=dst,
        send_sem=send_sem,
        recv_sem=recv_sem,
        device_id=device,
        device_id_type=MESH,
    )


def dot(a, b, contract=((1,), (0,))):
    return lax.dot_general(a, b, (contract, ((), ())), preferred_element_type=jnp.float32)


def layer_kernel(
    sizes,
    q_hbm,
    k_hbm,
    v_hbm,
    gate_hbm,
    res_hbm,
    wo_hbm,
    gain_ref,
    up_hbm,
    dn_hbm,
    out_ref,
    q_all,
    kv_all,
    gate_all,
    v_ones,
    top_s,
    acc_s,
    o_send,
    o_recv,
    lse_send,
    lse_recv,
    heads,
    res_all,
    wo_s,
    rsum,
    normed,
    up_all,
    dn_all,
    hidden,
    part,
    pair_recv,
    sum_send,
    sum_recv,
    local_sem,
    q_sem,
    kvu_sem,
    kvd_sem,
    gu_sem,
    gd_sem,
    o_sem,
    lse_sem,
    head_sem,
    res_sem,
    upy_sem,
    upu_sem,
    upd_sem,
    dnu_sem,
    dnd_sem,
    dny_sem,
    pair_sem,
    sum_sem,
):
    nz, ny, nx, nc = sizes
    z, y, x, c = (lax.axis_index(name) for name in ("z", "y", "x", "c"))
    tp = x * nc + c
    tok, hd = q_all.shape[1], q_all.shape[2]
    own_rows, width = out_ref.shape
    to_exp2 = hd**-0.5 * math.log2(math.e)
    kv_up, kv_down = nz // 2, nz - 1 - nz // 2
    w_up, w_down = nz - 1 - nz // 2, nz // 2
    tiles = ny * tok // ROW_TILE
    per_block = tok // ROW_TILE

    def wrap(value, size):
        return lax.rem(value + size, size)

    above, below = {"z": wrap(z + 1, nz)}, {"z": wrap(z - 1, nz)}

    def y_peer(d):
        return {"y": wrap(y + d, ny)}

    tp_peers = [(dx, dc) for dx in range(nx) for dc in range(nc) if dx or dc]

    def tp_peer(dx, dc):
        return {"x": wrap(x + dx, nx), "c": wrap(c + dc, nc)}

    def tp_from(dx, dc):
        return wrap(x - dx, nx) * nc + wrap(c - dc, nc)

    locals_ = [
        pltpu.make_async_copy(src, dst, local_sem.at[i])
        for i, (src, dst) in enumerate(
            [
                (k_hbm, kv_all.at[z, 0]),
                (v_hbm, kv_all.at[z, 1]),
                (gate_hbm, gate_all.at[z]),
                (q_hbm, q_all.at[y]),
                (up_hbm, up_all.at[z, y]),
                (dn_hbm, dn_all.at[z, y]),
                (res_hbm, res_all.at[tp]),
                (wo_hbm, wo_s),
            ]
        )
    ]
    for copy in locals_:
        copy.start()

    barrier = pltpu.get_barrier_semaphore()
    peers = [above, below] + [y_peer(d) for d in range(1, ny)]
    peers += [tp_peer(dx, dc) for dx, dc in tp_peers]
    for peer in peers:
        pl.semaphore_signal(barrier, inc=1, device_id=peer, device_id_type=MESH)
    pl.semaphore_wait(barrier, len(peers))

    def kv_copy(slot, sems, gate_sems, step, device):
        return (
            remote(kv_all.at[slot], kv_all.at[slot], sems.at[0, step - 1], sems.at[1, step - 1], device),
            remote(
                gate_all.at[slot],
                gate_all.at[slot],
                gate_sems.at[0, step - 1],
                gate_sems.at[1, step - 1],
                device,
            ),
        )

    def kv_up_send(step):
        slot = z - step + 1
        return (slot >= 0) & (z < nz - 1), kv_copy(wrap(slot, nz), kvu_sem, gu_sem, step, above)

    def kv_up_recv(step):
        return z - step >= 0, kv_copy(wrap(z - step, nz), kvu_sem, gu_sem, step, above)

    def kv_down_send(step):
        slot = wrap(z + step - 1, nz)
        return slot < kv_down, kv_copy(slot, kvd_sem, gd_sem, step, below)

    def kv_down_recv(step):
        slot = wrap(z + step, nz)
        return slot < kv_down, kv_copy(slot, kvd_sem, gd_sem, step, below)

    def start(pair):
        when, copies = pair

        @pl.when(when)
        def _():
            for copy in copies:
                copy.start()

    def wait_recv(pair):
        when, copies = pair

        @pl.when(when)
        def _():
            for copy in copies:
                copy.wait_recv()

    def wait_send(pair):
        when, copies = pair

        @pl.when(when)
        def _():
            for copy in copies:
                copy.wait_send()

    def ring(buf, sems, step, device, slot):
        return remote(buf.at[slot], buf.at[slot], sems.at[0, step - 1], sems.at[1, step - 1], device)

    def upu(step, arriving=False):
        return ring(up_all, upu_sem, step, above, wrap(z - step + (0 if arriving else 1), nz))

    def upd(step, arriving=False):
        return ring(up_all, upd_sem, step, below, wrap(z + step - (0 if arriving else 1), nz))

    def dn_ring(sems, step, device, slot):
        ref = dn_all.at[slot, y]
        return remote(ref, ref, sems.at[0, step - 1], sems.at[1, step - 1], device)

    def dnu(step, arriving=False):
        return dn_ring(dnu_sem, step, above, wrap(z - step + (0 if arriving else 1), nz))

    def dnd(step, arriving=False):
        return dn_ring(dnd_sem, step, below, wrap(z + step - (0 if arriving else 1), nz))

    def y_copies(buf_at, sems, arriving=False):
        out = []
        for d in range(1, ny):
            ref = buf_at(wrap(y - d, ny) if arriving else y)
            out.append(remote(ref, ref, sems.at[0, d - 1], sems.at[1, d - 1], y_peer(d)))
        return out

    def dny(k, arriving=False):
        slot = wrap(z + k, nz)
        row = k + w_up
        return y_copies(lambda at: dn_all.at[slot, at], dny_sem.at[row], arriving)

    q_send = y_copies(lambda at: q_all.at[at], q_sem)
    q_arrive = y_copies(lambda at: q_all.at[at], q_sem, True)
    upy_send = y_copies(lambda at: up_all.at[z, at], upy_sem)
    upy_arrive = y_copies(lambda at: up_all.at[z, at], upy_sem, True)

    def tp_copies(buf, sems, arriving=False):
        out = []
        for i, (dx, dc) in enumerate(tp_peers):
            ref = buf.at[tp_from(dx, dc) if arriving else tp]
            out.append(remote(ref, ref, sems.at[0, i], sems.at[1, i], tp_peer(dx, dc)))
        return out

    res_send, res_arrive = tp_copies(res_all, res_sem), tp_copies(res_all, res_sem, True)
    head_send, head_arrive = tp_copies(heads, head_sem), tp_copies(heads, head_sem, True)

    def o_copies(arriving=False):
        out = []
        for d in range(1, ny):
            to = wrap(y + d, ny)
            source = wrap(y - d, ny) if arriving else y
            out.append(
                remote(o_send.at[to], o_recv.at[source], o_sem.at[0, d - 1], o_sem.at[1, d - 1], y_peer(d))
            )
            out.append(
                remote(
                    lse_send.at[to], lse_recv.at[source], lse_sem.at[0, d - 1], lse_sem.at[1, d - 1], y_peer(d)
                )
            )
        return out

    def start_all(copies):
        for copy in copies:
            copy.start()

    for copy in locals_[:3]:
        copy.wait()
    start(kv_up_send(1))
    start(kv_down_send(1))
    locals_[3].wait()
    start_all(q_send)
    locals_[4].wait()
    start_all(upy_send)
    locals_[5].wait()
    dnd(1).start()
    start_all(dny(0))
    locals_[6].wait()
    start_all(res_send)

    top_s[...] = jnp.full_like(top_s, LOW)
    acc_s[...] = jnp.zeros_like(acc_s)
    v_ones[:, hd:] = jnp.ones((tok, hd), jnp.bfloat16)

    def attend(slot, first_tile, masked):
        v_ones[:, :hd] = kv_all[slot, 1]

        def tile(t, carry):
            rows = pl.ds(t * ROW_TILE, ROW_TILE)
            q = q_all[t // per_block, pl.ds(lax.rem(t, per_block) * ROW_TILE, ROW_TILE), :]
            s = dot(q, kv_all[slot, 0], ((1,), (1,))) - gate_all[slot, 0:1, :] * (hd**0.5)
            if masked:
                q_pos = t * ROW_TILE + lax.broadcasted_iota(jnp.int32, s.shape, 0)
                k_pos = y * tok + lax.broadcasted_iota(jnp.int32, s.shape, 1)
                s = jnp.where(k_pos <= q_pos, s, LOW)
            old = top_s[rows, :]
            new = jnp.maximum(old, jnp.max(s, axis=1, keepdims=True))
            fade = jnp.exp2((old - new) * to_exp2)
            weights = jnp.exp2((s - jnp.concatenate([new] * (tok // hd), axis=1)) * to_exp2)
            product = dot(weights.astype(jnp.bfloat16), v_ones[...])
            acc_s[rows, :] = acc_s[rows, :] * jnp.concatenate([fade, fade], axis=1) + product
            top_s[rows, :] = new
            return carry

        lax.fori_loop(first_tile, tiles, tile, 0)

    for copy in q_arrive:
        copy.wait_recv()
    attend(z, y * per_block, True)

    for step in range(1, kv_up + 1):
        wait_recv(kv_up_recv(step))
        if step < kv_up:
            start(kv_up_send(step + 1))
        if step <= kv_down:
            wait_recv(kv_down_recv(step))
            if step < kv_down:
                start(kv_down_send(step + 1))
        if step == 1:
            for copy in upy_arrive:
                copy.wait_recv()
            upd(1).start()
        if step == kv_up - 1:
            dnu(1).start()
            upu(1).start()

        @pl.when(z - step >= 0)
        def _():
            attend(wrap(z - step, nz), 0, False)

        if step <= kv_down:

            @pl.when(z + step >= nz)
            def _():
                attend(wrap(z + step, nz), 0, False)

        if step <= w_down:
            dnd(step, True).wait_recv()
            if step < w_down:
                dnd(step + 1).start()
            if step <= 2:
                start_all(dny(step))
    upd(1, True).wait_recv()
    upd(2).start()

    eye = lax.broadcasted_iota(jnp.int32, (hd, hd), 0) == lax.broadcasted_iota(jnp.int32, (hd, hd), 1)

    for block in range(ny):
        for sub in range(tok // hd):
            rows = pl.ds(block * tok + sub * hd, hd)
            denom = jnp.maximum(acc_s[rows, hd:], 1e-30)
            o_send[block, sub * hd : (sub + 1) * hd, :] = (acc_s[rows, :hd] / denom).astype(jnp.bfloat16)
            lse = top_s[rows, :] * to_exp2 + jnp.log2(denom)
            line = jnp.sum(jnp.where(eye, lse, 0.0), axis=0, keepdims=True)
            lse_send[block, :, sub * hd : (sub + 1) * hd] = jnp.broadcast_to(line, (8, hd))
    start_all(o_copies())
    o_recv[y] = o_send[y]
    lse_recv[y] = lse_send[y]

    for step in range(3, w_down + 1):
        start_all(dny(step))
    dnu(1, True).wait_recv()
    dnu(2).start()
    start_all(dny(-1))

    for copy in o_copies(True):
        copy.wait_recv()
    for sub in range(tok // hd):
        span = slice(sub * hd, (sub + 1) * hd)
        lines = [lse_recv[i, 0:1, span] for i in range(ny)]
        best = functools.reduce(jnp.maximum, lines)
        shares = [jnp.exp2(line - best) for line in lines]
        total = functools.reduce(jnp.add, shares)
        summed = jnp.zeros((hd, hd), jnp.float32)
        for i in range(ny):
            share = jnp.broadcast_to(shares[i] / total, (hd, hd))
            column = jnp.sum(jnp.where(eye, share, 0.0), axis=1, keepdims=True)
            summed = summed + column * o_recv[i, span, :].astype(jnp.float32)
        heads[tp, span, :] = summed.astype(jnp.bfloat16)
    start_all(head_send)

    dnu(2, True).wait_recv()
    dnu(3).start()
    start_all(dny(-2))
    upu(1, True).wait_recv()
    upu(2).start()
    upd(2, True).wait_recv()
    upd(3).start()

    locals_[7].wait()
    for copy in res_arrive:
        copy.wait_recv()
    for copy in head_arrive:
        copy.wait_recv()
    n_heads = heads.shape[0]

    def project(n, squares):
        cols = pl.ds(pl.multiple_of(n * COL_TILE, COL_TILE), COL_TILE)
        attended = jnp.concatenate([heads[h] for h in range(n_heads)], axis=1)
        base = res_all[:, :, cols].reshape(tok, COL_TILE).astype(jnp.float32)
        total = base + dot(attended, wo_s[:, cols])
        rsum[:, cols] = total
        return squares + jnp.sum(total * total, axis=1, keepdims=True)

    squares = lax.fori_loop(0, width // COL_TILE, project, jnp.zeros((tok, 1), jnp.float32))
    inverse = lax.rsqrt(squares / width + 1e-06)
    top_s[0:tok, :] = jnp.broadcast_to(inverse, (tok, hd))

    def normalise(r, carry):
        rows = pl.ds(pl.multiple_of(r * own_rows, own_rows), own_rows)
        factor = top_s[rows, 0:1]
        normed[rows, :] = (rsum[rows, :] * factor * gain_ref[...]).astype(jnp.bfloat16)
        return carry

    lax.fori_loop(0, tok // own_rows, normalise, 0)

    upu(2, True).wait_recv()
    upu(3).start()
    upd(3, True).wait_recv()
    upd(4).start()
    dnu(3, True).wait_recv()
    start_all(dny(-3))

    upu(3, True).wait_recv()
    upd(4, True).wait_recv()
    ff = hidden.shape[1]

    def up_tile(n, carry):
        cols = pl.ds(pl.multiple_of(n * COL_TILE, COL_TILE), COL_TILE)
        proj = dot(normed[...], up_all[:, :, :, cols].reshape(width, COL_TILE))
        hidden[:, cols] = jnp.square(jnp.maximum(proj, 0.0)).astype(jnp.bfloat16)
        return carry

    lax.fori_loop(0, ff // COL_TILE, up_tile, 0)

    for k in range(-w_up, w_down + 1):
        for copy in dny(k, True):
            copy.wait_recv()

    group_cols = width // GROUPS
    z_per_group = nz // GROUPS
    z_cols = width // nz

    def pair_copy(g):
        cols = slice(g * group_cols, (g + 1) * group_cols)
        return remote(
            part.at[1 - c, :, :, cols],
            pair_recv.at[:, :, cols],
            pair_sem.at[0, g],
            pair_sem.at[1, g],
            {"c": 1 - c},
        )

    def sum_copy(g, d):
        cols = slice(g * group_cols, (g + 1) * group_cols)
        return remote(
            sum_send.at[d, :, cols],
            sum_recv.at[d, :, cols],
            sum_sem.at[0, g, d - 1],
            sum_sem.at[1, g, d - 1],
            {"x": wrap(x + d, nx)},
        )

    def finish_pair(g):
        cols = slice(g * group_cols, (g + 1) * group_cols)
        pair_copy(g).wait_recv()
        for d in range(1, nx):
            at = wrap(x + d, nx)
            both = part[c, at, :, cols].astype(jnp.float32) + pair_recv[at, :, cols].astype(jnp.float32)
            sum_send[d, :, cols] = both.astype(jnp.bfloat16)
            sum_copy(g, d).start()

    for g in range(GROUPS):

        def down_tile(i, carry, g=g):
            at = g * z_per_group + i
            cols = pl.ds(pl.multiple_of(at * z_cols, z_cols), z_cols)
            block = dot(hidden[...], dn_all[at].reshape(z_cols, ff), ((1,), (1,)))
            for owner in range(nx * nc):
                part[owner % nc, owner // nc, :, cols] = block[
                    owner * own_rows : (owner + 1) * own_rows, :
                ].astype(jnp.bfloat16)
            return carry

        lax.fori_loop(0, z_per_group, down_tile, 0)
        pair_copy(g).start()
        if g:
            finish_pair(g - 1)
    finish_pair(GROUPS - 1)

    final = rsum[pl.ds(pl.multiple_of(tp * own_rows, own_rows), own_rows), :]
    final = final + (part[c, x].astype(jnp.float32) + pair_recv[x].astype(jnp.float32))
    for g in range(GROUPS):
        for d in range(1, nx):
            sum_copy(g, d).wait_recv()
    for d in range(1, nx):
        final = final + sum_recv[d].astype(jnp.float32)
    out_ref[...] = final.astype(jnp.bfloat16)

    for step in range(1, kv_up + 1):
        wait_send(kv_up_send(step))
    for step in range(1, kv_down + 1):
        wait_send(kv_down_send(step))
    sent = q_send + upy_send + res_send + head_send + o_copies()
    for step in range(1, w_up + 1):
        sent += [upu(step), dnu(step)]
    for step in range(1, w_down + 1):
        sent += [upd(step), dnd(step)]
    for k in range(-w_up, w_down + 1):
        sent += dny(k)
    for g in range(GROUPS):
        sent += [pair_copy(g)] + [sum_copy(g, d) for d in range(1, nx)]
    for copy in sent:
        copy.wait_send()


def per_device(sizes, queries, keys, values, cum_gate, residual, w_out, gain, w_up, w_down):
    nz, ny, nx, nc = sizes
    ntp = nx * nc
    tok, hd = queries.shape
    rows, width = residual.shape
    depth, ff = w_up.shape
    gates = jnp.broadcast_to(cum_gate.reshape(1, tok), (8, tok))
    bf16, f32 = jnp.bfloat16, jnp.float32
    anywhere = pl.BlockSpec(memory_space=pl.ANY)
    in_vmem = pl.BlockSpec(memory_space=pltpu.VMEM)
    dma = pltpu.SemaphoreType.DMA
    up_steps, down_steps = nz // 2, nz - 1 - nz // 2
    return pl.pallas_call(
        functools.partial(layer_kernel, sizes),
        out_shape=jax.ShapeDtypeStruct((rows, width), bf16),
        in_specs=[anywhere] * 6 + [in_vmem] + [anywhere] * 2,
        out_specs=in_vmem,
        scratch_shapes=[
            pltpu.VMEM((ny, tok, hd), bf16),
            pltpu.VMEM((nz, 2, tok, hd), bf16),
            pltpu.VMEM((nz, 8, tok), f32),
            pltpu.VMEM((tok, 2 * hd), bf16),
            pltpu.VMEM((ny * tok, hd), f32),
            pltpu.VMEM((ny * tok, 2 * hd), f32),
            pltpu.VMEM((ny, tok, hd), bf16),
            pltpu.VMEM((ny, tok, hd), bf16),
            pltpu.VMEM((ny, 8, tok), f32),
            pltpu.VMEM((ny, 8, tok), f32),
            pltpu.VMEM((ntp, tok, hd), bf16),
            pltpu.VMEM((ntp, rows, width), bf16),
            pltpu.VMEM(w_out.shape, bf16),
            pltpu.VMEM((tok, width), f32),
            pltpu.VMEM((tok, width), bf16),
            pltpu.VMEM((nz, ny, depth, ff), bf16),
            pltpu.VMEM((nz, ny, depth, ff), bf16),
            pltpu.VMEM((tok, ff), bf16),
            pltpu.VMEM((nc, nx, rows, width), bf16),
            pltpu.VMEM((nx, rows, width), bf16),
            pltpu.VMEM((nx, rows, width), bf16),
            pltpu.VMEM((nx, rows, width), bf16),
            dma((8,)),
            dma((2, ny - 1)),
            dma((2, up_steps)),
            dma((2, down_steps)),
            dma((2, up_steps)),
            dma((2, down_steps)),
            dma((2, ny - 1)),
            dma((2, ny - 1)),
            dma((2, ntp - 1)),
            dma((2, ntp - 1)),
            dma((2, ny - 1)),
            dma((2, down_steps)),
            dma((2, up_steps)),
            dma((2, down_steps)),
            dma((2, up_steps)),
            dma((nz, 2, ny - 1)),
            dma((2, GROUPS)),
            dma((2, GROUPS, nx - 1)),
        ],
        compiler_params=pltpu.CompilerParams(
            collective_id=0, has_side_effects=True, vmem_limit_bytes=63 * 1024 * 1024
        ),
    )(queries, keys, values, gates, residual, w_out, gain.reshape(1, width), w_up, w_down.T)


def solution(mesh):
    finer = Mesh(mesh.devices.reshape(GRID), ("z", "y", "x", "c"))
    sp, tp = ("z", "y"), ("x", "c")
    rows = ("z", "y", "x", "c")
    in_specs = (
        P(sp, tp),
        P(sp, tp),
        P(sp, tp),
        P(sp, tp),
        P(rows, None),
        P(),
        P(),
        P(sp, tp),
        P(tp, sp),
    )
    return jax.shard_map(
        functools.partial(per_device, GRID),
        mesh=finer,
        in_specs=in_specs,
        out_specs=P(rows, None),
        check_vma=False,
    )
```

```python
import functools
import math

import jax
import jax.numpy as jnp
from jax import lax
from jax.experimental import pallas as pl
from jax.experimental.pallas import tpu as pltpu
from jax.sharding import Mesh
from jax.sharding import PartitionSpec as P

MESH = pl.DeviceIdType.MESH
GRID = (8, 4, 4, 2)
ROW_TILE = 256
COL_TILE = 256
FIRST_ROWS = 32
LOW = -1e30


def remote(src, dst, send_sem, recv_sem, device):
    return pltpu.make_async_remote_copy(
        src_ref=src,
        dst_ref=dst,
        send_sem=send_sem,
        recv_sem=recv_sem,
        device_id=device,
        device_id_type=MESH,
    )


def dot(a, b, contract=((1,), (0,))):
    return lax.dot_general(a, b, (contract, ((), ())), preferred_element_type=jnp.float32)


def layer_kernel(
    sizes,
    q_hbm,
    k_hbm,
    v_hbm,
    gate_hbm,
    res_hbm,
    wo_hbm,
    gain_ref,
    up_hbm,
    dn_hbm,
    out_ref,
    q_all,
    kv_all,
    gate_all,
    v_ones,
    top_s,
    acc_s,
    o_send,
    o_recv,
    lse_send,
    lse_recv,
    heads,
    res_all,
    wo_s,
    rsum,
    normed,
    up_all,
    dn_all,
    hidden,
    part,
    pair_recv,
    sum_send,
    sum_recv,
    local_sem,
    q_sem,
    kvu_sem,
    kvd_sem,
    gu_sem,
    gd_sem,
    vu_sem,
    vd_sem,
    o_sem,
    lse_sem,
    head_sem,
    pair_head_sem,
    res_sem,
    upy_sem,
    upu_sem,
    upd_sem,
    dnu_sem,
    dnd_sem,
    dny_sem,
    dnh_sem,
    u2u_sem,
    u2d_sem,
    u2y_sem,
    u2h_sem,
    pair_sem,
    sum_sem,
):
    nz, ny, nx, nc = sizes
    z, y, x, c = (lax.axis_index(name) for name in ("z", "y", "x", "c"))
    tp = x * nc + c
    tok, hd = q_all.shape[1], q_all.shape[2]
    own_rows, width = out_ref.shape
    to_exp2 = hd**-0.5 * math.log2(math.e)
    kv_up, kv_down = nz // 2, nz - 1 - nz // 2
    w_up, w_down = nz - 1 - nz // 2, nz // 2
    tiles = ny * tok // ROW_TILE
    per_block = tok // ROW_TILE

    def wrap(value, size):
        return lax.rem(value + size, size)

    above, below = {"z": wrap(z + 1, nz)}, {"z": wrap(z - 1, nz)}

    def y_peer(d):
        return {"y": wrap(y + d, ny)}

    tp_peers = [(dx, dc) for dx in range(nx) for dc in range(nc) if dx or dc]

    def tp_peer(dx, dc):
        return {"x": wrap(x + dx, nx), "c": wrap(c + dc, nc)}

    def tp_from(dx, dc):
        return wrap(x - dx, nx) * nc + wrap(c - dc, nc)

    locals_ = [
        pltpu.make_async_copy(src, dst, local_sem.at[i])
        for i, (src, dst) in enumerate(
            [
                (k_hbm, kv_all.at[z, 0]),
                (v_hbm, kv_all.at[z, 1]),
                (gate_hbm, gate_all.at[z]),
                (q_hbm, q_all.at[y]),
                (up_hbm, up_all.at[z, y]),
                (dn_hbm, dn_all.at[z, y]),
                (res_hbm, res_all.at[tp]),
                (wo_hbm, wo_s),
            ]
        )
    ]
    for copy in locals_:
        copy.start()

    barrier = pltpu.get_barrier_semaphore()
    peers = [above, below] + [y_peer(d) for d in range(1, ny)]
    peers += [tp_peer(dx, dc) for dx, dc in tp_peers]
    for peer in peers:
        pl.semaphore_signal(barrier, inc=1, device_id=peer, device_id_type=MESH)
    pl.semaphore_wait(barrier, len(peers))

    def kv_copy(which, slot, up, step, device):
        ref = kv_all.at[slot, which]
        sems = ((kvu_sem, vu_sem) if up else (kvd_sem, vd_sem))[which]
        copies = (remote(ref, ref, sems.at[0, step - 1], sems.at[1, step - 1], device),)
        if which == 0:
            ref, sems = gate_all.at[slot], gu_sem if up else gd_sem
            copies += (remote(ref, ref, sems.at[0, step - 1], sems.at[1, step - 1], device),)
        return copies

    def kv_up_send(which, step):
        slot = z - step + 1
        return (slot >= 0) & (z < nz - 1), kv_copy(which, wrap(slot, nz), True, step, above)

    def kv_up_recv(which, step):
        return z - step >= 0, kv_copy(which, wrap(z - step, nz), True, step, above)

    def kv_down_send(which, step):
        slot = wrap(z + step - 1, nz)
        return slot < kv_down, kv_copy(which, slot, False, step, below)

    def kv_down_recv(which, step):
        slot = wrap(z + step, nz)
        return slot < kv_down, kv_copy(which, slot, False, step, below)

    def start(pair):
        when, copies = pair

        @pl.when(when)
        def _():
            for copy in copies:
                copy.start()

    def wait_recv(pair):
        when, copies = pair

        @pl.when(when)
        def _():
            for copy in copies:
                copy.wait_recv()

    def wait_send(pair):
        when, copies = pair

        @pl.when(when)
        def _():
            for copy in copies:
                copy.wait_send()

    def up_ring(sems, d, step, device, slot):
        ref = up_all.at[slot, wrap(y - d, ny), 0:FIRST_ROWS, :]
        return remote(ref, ref, sems.at[0, step - 1, d], sems.at[1, step - 1, d], device)

    def upu(d, step, arriving=False):
        return up_ring(upu_sem, d, step, above, wrap(z - step + (0 if arriving else 1), nz))

    def upd(d, step, arriving=False):
        return up_ring(upd_sem, d, step, below, wrap(z + step - (0 if arriving else 1), nz))

    def pass_upu(d, step):
        upu(d, step, True).wait_recv()
        if step < w_up:
            upu(d, step + 1).start()

    def pass_upd(d, step):
        upd(d, step, True).wait_recv()
        if step < w_down:
            upd(d, step + 1).start()

    def pass_dnu(step):
        for copy in dnu(step, True):
            copy.wait_recv()
        if step < w_up:
            start_all(dnu(step + 1))

    def pass_dnd(step):
        for copy in dnd(step, True):
            copy.wait_recv()
        if step < w_down:
            start_all(dnd(step + 1))

    def rest_ring(sems, rest_sems, step, device, slot):
        out = []
        for ref, s in ((dn_all.at[slot, y], sems), (up_all.at[slot, y, FIRST_ROWS:, :], rest_sems)):
            out.append(remote(ref, ref, s.at[0, step - 1], s.at[1, step - 1], device))
        return out

    def dnu(step, arriving=False):
        slot = wrap(z - step + (0 if arriving else 1), nz)
        return rest_ring(dnu_sem, u2u_sem, step, above, slot)

    def dnd(step, arriving=False):
        slot = wrap(z + step - (0 if arriving else 1), nz)
        return rest_ring(dnd_sem, u2d_sem, step, below, slot)

    def y_copies(buf_at, sems, arriving=False):
        out = []
        for d in range(1, ny):
            ref = buf_at(wrap(y - d, ny) if arriving else y)
            out.append(remote(ref, ref, sems.at[0, d - 1], sems.at[1, d - 1], y_peer(d)))
        return out

    rest_rows = slice(FIRST_ROWS, up_all.shape[2])

    def over_y(rest, k, side, arriving=False, half=False):
        buf, rows = (up_all, rest_rows) if rest else (dn_all, slice(0, dn_all.shape[2]))
        i = (1 - side) // 2
        source = y - side * ((1 if half else 0) + (1 if arriving else 0))
        if half:
            mid = (rows.start + rows.stop) // 2
            rows = slice(mid, rows.stop) if i else slice(rows.start, mid)
        ref = buf.at[wrap(z + k, nz), wrap(source, ny), rows, :]
        sems = (u2h_sem if rest else dnh_sem) if half else (u2y_sem if rest else dny_sem)
        sems = sems.at[k + w_up]
        return remote(ref, ref, sems.at[0, i], sems.at[1, i], y_peer(side))

    def send_y(k):
        for rest in (True, False):
            for side in (1, -1):
                over_y(rest, k, side).start()

    def pass_y(k):
        for rest in (True, False):
            for side in (1, -1):
                over_y(rest, k, side, True).wait_recv()
                over_y(rest, k, side, half=True).start()

    q_send = y_copies(lambda at: q_all.at[at], q_sem)
    q_arrive = y_copies(lambda at: q_all.at[at], q_sem, True)
    upy_send = y_copies(lambda at: up_all.at[z, at, 0:FIRST_ROWS, :], upy_sem)
    upy_arrive = y_copies(lambda at: up_all.at[z, at, 0:FIRST_ROWS, :], upy_sem, True)

    def tp_copies(buf, sems, arriving=False):
        out = []
        for i, (dx, dc) in enumerate(tp_peers):
            ref = buf.at[tp_from(dx, dc) if arriving else tp]
            out.append(remote(ref, ref, sems.at[0, i], sems.at[1, i], tp_peer(dx, dc)))
        return out

    res_send, res_arrive = tp_copies(res_all, res_sem), tp_copies(res_all, res_sem, True)

    def head_copy(d, arriving=False):
        ref = heads.at[wrap(x - d, nx) * nc + c if arriving else tp]
        return remote(ref, ref, head_sem.at[0, d - 1], head_sem.at[1, d - 1], {"x": wrap(x + d, nx)})

    def head_to_pair(d, arriving=False):
        ref = heads.at[wrap(x - d, nx) * nc + (1 - c if arriving else c)]
        return remote(ref, ref, pair_head_sem.at[0, d], pair_head_sem.at[1, d], {"c": 1 - c})

    def o_copies(arriving=False):
        out = []
        for d in range(1, ny):
            to = wrap(y + d, ny)
            source = wrap(y - d, ny) if arriving else y
            out.append(
                remote(o_send.at[to], o_recv.at[source], o_sem.at[0, d - 1], o_sem.at[1, d - 1], y_peer(d))
            )
            out.append(
                remote(
                    lse_send.at[to], lse_recv.at[source], lse_sem.at[0, d - 1], lse_sem.at[1, d - 1], y_peer(d)
                )
            )
        return out

    def start_all(copies):
        for copy in copies:
            copy.start()

    locals_[0].wait()
    locals_[2].wait()
    start(kv_up_send(0, 1))
    start(kv_down_send(0, 1))
    locals_[1].wait()
    start(kv_up_send(1, 1))
    start(kv_down_send(1, 1))
    locals_[3].wait()
    start_all(q_send)
    locals_[4].wait()
    locals_[5].wait()
    start_all(dnd(1))
    start_all(dnu(1))
    upd(0, 1).start()
    start_all(upy_send)
    send_y(0)
    locals_[6].wait()
    start_all(res_send)

    top_s[...] = jnp.full_like(top_s, LOW)
    acc_s[...] = jnp.zeros_like(acc_s)
    v_ones[:, hd:] = jnp.ones((tok, hd), jnp.bfloat16)

    def attend(slot, first_tile, count, masked=False):
        for t in [first_tile + u for u in range(count)]:
            rows = pl.ds(t * ROW_TILE, ROW_TILE)
            q = q_all[t // per_block, pl.ds(lax.rem(t, per_block) * ROW_TILE, ROW_TILE), :]
            s = dot(q, kv_all[slot, 0], ((1,), (1,))) - gate_all[slot] * (hd**0.5)
            if masked:
                q_pos = t * ROW_TILE + lax.broadcasted_iota(jnp.int32, s.shape, 0)
                k_pos = y * tok + lax.broadcasted_iota(jnp.int32, s.shape, 1)
                s = jnp.where(k_pos <= q_pos, s, LOW)
            old = top_s[rows, :]
            new = jnp.maximum(old, jnp.max(s, axis=1, keepdims=True))
            fade = jnp.exp2((old - new) * to_exp2)
            weights = jnp.exp2((s - jnp.concatenate([new] * (tok // hd), axis=1)) * to_exp2)
            product = dot(weights.astype(jnp.bfloat16), v_ones[...])
            acc_s[rows, :] = acc_s[rows, :] * jnp.concatenate([fade, fade], axis=1) + product
            top_s[rows, :] = new

    v_ones[:, :hd] = kv_all[z, 1]
    attend(z, y * per_block, per_block, True)
    for copy in q_arrive:
        copy.wait_recv()

    def later_block(b, carry):
        attend(z, b * per_block, per_block)
        return carry

    lax.fori_loop(y + 1, ny, later_block, 0)

    def forward_kv(step):
        for which in range(2):
            wait_recv(kv_up_recv(which, step))
            if step < kv_up:
                start(kv_up_send(which, step + 1))
            if step <= kv_down:
                wait_recv(kv_down_recv(which, step))
                if step < kv_down:
                    start(kv_down_send(which, step + 1))

    def attend_step(step):
        first = jnp.where(z - step >= 0, 0, 1)
        last = jnp.where(z + step >= nz, 2, 1) if step <= kv_down else 1

        def block(u, carry):
            slot = wrap(z + (2 * u - 1) * step, nz)
            v_ones[:, :hd] = kv_all[slot, 1]
            attend(slot, 0, tiles)
            return carry

        lax.fori_loop(first, last, block, 0)

    forward_kv(1)
    for d in range(1, ny):
        upy_arrive[d - 1].wait_recv()
        upd(d, 1).start()
    attend_step(1)
    pass_dnd(1)
    pass_dnu(1)
    send_y(1)
    send_y(-1)
    pass_y(0)

    forward_kv(2)
    pass_upd(0, 1)
    attend_step(2)
    pass_dnd(2)
    pass_dnu(2)
    send_y(2)
    send_y(-2)
    pass_y(1)

    forward_kv(3)
    for d in range(ny):
        upu(d, 1).start()
    pass_upd(1, 1)
    attend_step(3)
    pass_upd(2, 1)
    pass_dnd(3)
    pass_dnu(3)
    pass_y(-1)

    forward_kv(4)
    pass_upd(3, 1)
    pass_upd(0, 2)
    attend_step(4)
    pass_upd(1, 2)
    pass_upd(2, 2)
    pass_y(2)

    eye = lax.broadcasted_iota(jnp.int32, (hd, hd), 0) == lax.broadcasted_iota(jnp.int32, (hd, hd), 1)

    for block in range(ny):
        for sub in range(tok // hd):
            rows = pl.ds(block * tok + sub * hd, hd)
            denom = jnp.maximum(acc_s[rows, hd:], 1e-30)
            o_send[block, sub * hd : (sub + 1) * hd, :] = (acc_s[rows, :hd] / denom).astype(jnp.bfloat16)
            lse = top_s[rows, :] * to_exp2 + jnp.log2(denom)
            line = jnp.sum(jnp.where(eye, lse, 0.0), axis=0, keepdims=True)
            lse_send[block, :, sub * hd : (sub + 1) * hd] = line
    start_all(o_copies())
    o_recv[y] = o_send[y]
    lse_recv[y] = lse_send[y]

    pass_dnd(4)
    for k in (3, -3, 4):
        send_y(k)
    pass_y(-2)
    pass_upu(0, 1)
    pass_upu(1, 1)
    pass_upd(3, 2)

    for copy in o_copies(True):
        copy.wait_recv()
    for sub in range(tok // hd):
        span = slice(sub * hd, (sub + 1) * hd)
        lines = [lse_recv[i, 0:1, span] for i in range(ny)]
        best = functools.reduce(jnp.maximum, lines)
        shares = [jnp.exp2(line - best) for line in lines]
        total = functools.reduce(jnp.add, shares)
        summed = jnp.zeros((hd, hd), jnp.float32)
        for i in range(ny):
            share = jnp.broadcast_to(shares[i] / total, (hd, hd))
            column = jnp.sum(jnp.where(eye, share, 0.0), axis=1, keepdims=True)
            summed = summed + column * o_recv[i, span, :].astype(jnp.float32)
        heads[tp, span, :] = summed.astype(jnp.bfloat16)
    for d in range(1, nx):
        head_copy(d).start()
    head_to_pair(0).start()

    pass_upu(2, 1)
    pass_upu(3, 1)
    pass_upd(0, 3)
    pass_upd(1, 3)
    pass_y(3)

    locals_[7].wait()
    for copy in res_arrive:
        copy.wait_recv()
    for d in range(1, nx):
        head_copy(d, True).wait_recv()
        head_to_pair(d).start()
    pass_upu(0, 2)
    pass_upd(2, 3)
    pass_y(-3)
    for d in range(nx):
        head_to_pair(d, True).wait_recv()
    n_heads = heads.shape[0]

    def project(n, squares):
        cols = pl.ds(pl.multiple_of(n * COL_TILE, COL_TILE), COL_TILE)
        attended = jnp.concatenate([heads[h] for h in range(n_heads)], axis=1)
        base = res_all[:, :, cols].reshape(tok, COL_TILE).astype(jnp.float32)
        total = base + dot(attended, wo_s[:, cols])
        rsum[:, cols] = total
        return squares + jnp.sum(total * total, axis=1, keepdims=True)

    squares = jnp.zeros((tok, 1), jnp.float32)
    segment = width // COL_TILE // 4
    for i in range(4):
        squares = lax.fori_loop(i * segment, (i + 1) * segment, project, squares)
        if i < 3:
            pass_upu(i + 1, 2)
        else:
            pass_upd(3, 3)
    inverse = lax.rsqrt(squares / width + 1e-06)
    top_s[0:tok, :] = jnp.broadcast_to(inverse, (tok, hd))

    def normalise(r, carry):
        rows = pl.ds(pl.multiple_of(r * own_rows, own_rows), own_rows)
        factor = top_s[rows, 0:1]
        normed[rows, :] = (rsum[rows, :] * factor * gain_ref[...]).astype(jnp.bfloat16)
        return carry

    lax.fori_loop(0, tok // own_rows, normalise, 0)

    pass_y(4)

    for k in range(-w_up, w_down + 1):
        for side in (1, -1):
            over_y(True, k, side, True, True).wait_recv()
    for d in range(ny):
        pass_upu(d, 3)
        pass_upd(d, 4)
    ff = hidden.shape[1]

    def up_tile(n, carry):
        cols = pl.ds(pl.multiple_of(n * COL_TILE, COL_TILE), COL_TILE)
        proj = dot(normed[...], up_all[:, :, :, cols].reshape(width, COL_TILE))
        hidden[:, cols] = jnp.square(jnp.maximum(proj, 0.0)).astype(jnp.bfloat16)
        return carry

    lax.fori_loop(0, ff // COL_TILE, up_tile, 0)

    z_cols = width // nz
    order = [0] + [s for k in range(1, w_up + 1) for s in (k, -k)] + list(range(w_up + 1, w_down + 1))

    def cols_of(k):
        return pl.ds(pl.multiple_of(wrap(z + k, nz) * z_cols, z_cols), z_cols)

    def pair_copy(k):
        return remote(
            part.at[1 - c, :, :, cols_of(k)],
            pair_recv.at[:, :, cols_of(k)],
            pair_sem.at[0, k + w_up],
            pair_sem.at[1, k + w_up],
            {"c": 1 - c},
        )

    def sum_copy(k, d):
        return remote(
            sum_send.at[d, :, cols_of(k)],
            sum_recv.at[d, :, cols_of(k)],
            sum_sem.at[0, k + w_up, d - 1],
            sum_sem.at[1, k + w_up, d - 1],
            {"x": wrap(x + d, nx)},
        )

    def finish_pair(k):
        cols = cols_of(k)
        pair_copy(k).wait_recv()
        for d in range(1, nx):
            at = wrap(x + d, nx)
            both = part[c, at, :, cols].astype(jnp.float32) + pair_recv[at, :, cols].astype(jnp.float32)
            sum_send[d, :, cols] = both.astype(jnp.bfloat16)
            sum_copy(k, d).start()

    for i, k in enumerate(order):
        for side in (1, -1):
            over_y(False, k, side, True, True).wait_recv()
        block = dot(hidden[...], dn_all[wrap(z + k, nz)].reshape(z_cols, ff), ((1,), (1,)))
        for owner in range(nx * nc):
            part[owner % nc, owner // nc, :, cols_of(k)] = block[
                owner * own_rows : (owner + 1) * own_rows, :
            ].astype(jnp.bfloat16)
        pair_copy(k).start()
        if i:
            finish_pair(order[i - 1])
    finish_pair(order[-1])

    final = rsum[pl.ds(pl.multiple_of(tp * own_rows, own_rows), own_rows), :]
    final = final + (part[c, x].astype(jnp.float32) + pair_recv[x].astype(jnp.float32))
    for k in order:
        for d in range(1, nx):
            sum_copy(k, d).wait_recv()
    for d in range(1, nx):
        final = final + sum_recv[d].astype(jnp.float32)
    out_ref[...] = final.astype(jnp.bfloat16)

    for which in range(2):
        for step in range(1, kv_up + 1):
            wait_send(kv_up_send(which, step))
        for step in range(1, kv_down + 1):
            wait_send(kv_down_send(which, step))
    sent = q_send + upy_send + res_send + o_copies()
    sent += [head_copy(d) for d in range(1, nx)] + [head_to_pair(d) for d in range(nx)]
    for step in range(1, w_up + 1):
        sent += dnu(step) + [upu(d, step) for d in range(ny)]
    for step in range(1, w_down + 1):
        sent += dnd(step) + [upd(d, step) for d in range(ny)]
    for k in order:
        for rest in (True, False):
            for side in (1, -1):
                sent += [over_y(rest, k, side), over_y(rest, k, side, half=True)]
        sent += [pair_copy(k)] + [sum_copy(k, d) for d in range(1, nx)]
    for copy in sent:
        copy.wait_send()


def per_device(sizes, queries, keys, values, cum_gate, residual, w_out, gain, w_up, w_down):
    nz, ny, nx, nc = sizes
    ntp = nx * nc
    tok, hd = queries.shape
    rows, width = residual.shape
    depth, ff = w_up.shape
    gates = cum_gate.reshape(1, tok)
    bf16, f32 = jnp.bfloat16, jnp.float32
    anywhere = pl.BlockSpec(memory_space=pl.ANY)
    in_vmem = pl.BlockSpec(memory_space=pltpu.VMEM)
    dma = pltpu.SemaphoreType.DMA
    up_steps, down_steps = nz // 2, nz - 1 - nz // 2
    return pl.pallas_call(
        functools.partial(layer_kernel, sizes),
        out_shape=jax.ShapeDtypeStruct((rows, width), bf16),
        in_specs=[anywhere] * 6 + [in_vmem] + [anywhere] * 2,
        out_specs=in_vmem,
        scratch_shapes=[
            pltpu.VMEM((ny, tok, hd), bf16),
            pltpu.VMEM((nz, 2, tok, hd), bf16),
            pltpu.VMEM((nz, 1, tok), f32),
            pltpu.VMEM((tok, 2 * hd), bf16),
            pltpu.VMEM((ny * tok, hd), f32),
            pltpu.VMEM((ny * tok, 2 * hd), f32),
            pltpu.VMEM((ny, tok, hd), bf16),
            pltpu.VMEM((ny, tok, hd), bf16),
            pltpu.VMEM((ny, 1, tok), f32),
            pltpu.VMEM((ny, 1, tok), f32),
            pltpu.VMEM((ntp, tok, hd), bf16),
            pltpu.VMEM((ntp, rows, width), bf16),
            pltpu.VMEM(w_out.shape, bf16),
            pltpu.VMEM((tok, width), f32),
            pltpu.VMEM((tok, width), bf16),
            pltpu.VMEM((nz, ny, depth, ff), bf16),
            pltpu.VMEM((nz, ny, depth, ff), bf16),
            pltpu.VMEM((tok, ff), bf16),
            pltpu.VMEM((nc, nx, rows, width), bf16),
            pltpu.VMEM((nx, rows, width), bf16),
            pltpu.VMEM((nx, rows, width), bf16),
            pltpu.VMEM((nx, rows, width), bf16),
            dma((8,)),
            dma((2, ny - 1)),
            dma((2, up_steps)),
            dma((2, down_steps)),
            dma((2, up_steps)),
            dma((2, down_steps)),
            dma((2, up_steps)),
            dma((2, down_steps)),
            dma((2, ny - 1)),
            dma((2, ny - 1)),
            dma((2, nx - 1)),
            dma((2, nx)),
            dma((2, ntp - 1)),
            dma((2, ny - 1)),
            dma((2, down_steps, ny)),
            dma((2, up_steps, ny)),
            dma((2, down_steps)),
            dma((2, up_steps)),
            dma((nz, 2, 2)),
            dma((nz, 2, 2)),
            dma((2, down_steps)),
            dma((2, up_steps)),
            dma((nz, 2, 2)),
            dma((nz, 2, 2)),
            dma((2, nz)),
            dma((2, nz, nx - 1)),
        ],
        compiler_params=pltpu.CompilerParams(
            collective_id=0, has_side_effects=True, vmem_limit_bytes=63 * 1024 * 1024
        ),
    )(queries, keys, values, gates, residual, w_out, gain.reshape(1, width), w_up, w_down.T)


def solution(mesh):
    finer = Mesh(mesh.devices.reshape(GRID), ("z", "y", "x", "c"))
    sp, tp = ("z", "y"), ("x", "c")
    rows = ("z", "y", "x", "c")
    in_specs = (
        P(sp, tp),
        P(sp, tp),
        P(sp, tp),
        P(sp, tp),
        P(rows, None),
        P(),
        P(),
        P(sp, tp),
        P(tp, sp),
    )
    return jax.shard_map(
        functools.partial(per_device, GRID),
        mesh=finer,
        in_specs=in_specs,
        out_specs=P(rows, None),
        check_vma=False,
    )
```

```python
import functools
import math

import jax
import jax.numpy as jnp
from jax import lax
from jax.experimental import pallas as pl
from jax.experimental.pallas import tpu as pltpu
from jax.sharding import Mesh
from jax.sharding import PartitionSpec as P

MESH = pl.DeviceIdType.MESH
GRID = (8, 4, 4, 2)
ROW_TILE = 256
COL_TILE = 256
FIRST_ROWS = 32
LOW = -1e30

PLAN = {
    0: [],
    1: [("spread", 0, 1), ("down1", 0)],
    2: [],
    3: [("down1", 1)],
    4: [("ring", 1), ("ring", -1), ("spread", 0, 0), ("spread", 1, 0), ("spread", -1, 1), ("ring", -2), ("spread", -2, 0), ("spread", -1, 0)],
    5: [("down", 0, 1), ("down1", 2), ("relay", 0, 0), ("spread", 1, 1), ("relay", 1, 0)],
    6: [("ring", 2), ("up1", 1), ("spread", 2, 0), ("down", 2, 1), ("spread", -2, 1)],
    7: [("relay", -1, 1), ("spread", 2, 1), ("up", 1, 1)],
    8: [],
    9: [("relay", 0, 1), ("down", 1, 1), ("ring", 3), ("down1", 3), ("up1", 3)],
    10: [("down", 0, 2), ("up", 1, 2)],
    11: [("up1", 2), ("relay", 2, 1), ("down", 3, 1), ("up", 3, 1), ("ring", -3), ("ring", 4), ("spread", 3, 1), ("up1", 0), ("down", 2, 2), ("spread", -3, 1), ("relay", -2, 1)],
    12: [("spread", 4, 1), ("down", 3, 2), ("relay", 3, 1), ("up", 0, 1), ("down", 0, 3), ("spread", 3, 0), ("up", 3, 2), ("down", 1, 2), ("up", 2, 1), ("up", 0, 2)],
    13: [("relay", 4, 1), ("relay", 1, 1), ("relay", -3, 1), ("down", 2, 3), ("down", 1, 3), ("down", 3, 3), ("relay", -1, 0), ("down", 0, 4)],
    14: [],
    15: [("up", 2, 2), ("spread", -3, 0), ("up", 1, 3), ("relay", 3, 0)],
    16: [("relay", -2, 0), ("down", 2, 4)],
    17: [],
    18: [],
    19: [("down", 3, 4), ("relay", 2, 0), ("up", 2, 3), ("up", 3, 3), ("up", 0, 3), ("down", 1, 4)],
    20: [("spread", 4, 0)],
    21: [],
    22: [],
    23: [("relay", -3, 0)],
    24: [],
    25: [("relay", 4, 0)],
    26: [],
    27: [],
}


def remote(src, dst, send_sem, recv_sem, device):
    return pltpu.make_async_remote_copy(
        src_ref=src,
        dst_ref=dst,
        send_sem=send_sem,
        recv_sem=recv_sem,
        device_id=device,
        device_id_type=MESH,
    )


def dot(a, b, contract=((1,), (0,))):
    return lax.dot_general(a, b, (contract, ((), ())), preferred_element_type=jnp.float32)


def layer_kernel(
    sizes,
    q_hbm,
    k_hbm,
    v_hbm,
    gate_hbm,
    res_hbm,
    wo_hbm,
    gain_ref,
    up_hbm,
    dn_hbm,
    out_ref,
    q_all,
    kv_all,
    gate_all,
    v_ones,
    top_s,
    acc_s,
    o_send,
    o_recv,
    lse_send,
    lse_recv,
    heads,
    res_all,
    wo_s,
    rsum,
    normed,
    up_all,
    dn_all,
    hidden,
    part,
    pair_recv,
    sum_send,
    sum_recv,
    local_sem,
    q_sem,
    kvu_sem,
    kvd_sem,
    gu_sem,
    gd_sem,
    vu_sem,
    vd_sem,
    o_sem,
    lse_sem,
    head_sem,
    pair_head_sem,
    res_sem,
    upy_sem,
    upu_sem,
    upd_sem,
    dnu_sem,
    dnd_sem,
    dny_sem,
    dnh_sem,
    u2u_sem,
    u2d_sem,
    u2y_sem,
    u2h_sem,
    pair_sem,
    sum_sem,
):
    nz, ny, nx, nc = sizes
    z, y, x, c = (lax.axis_index(name) for name in ("z", "y", "x", "c"))
    tp = x * nc + c
    tok, hd = q_all.shape[1], q_all.shape[2]
    own_rows, width = out_ref.shape
    to_exp2 = hd**-0.5 * math.log2(math.e)
    kv_up, kv_down = nz // 2, nz - 1 - nz // 2
    w_up, w_down = nz - 1 - nz // 2, nz // 2
    tiles = ny * tok // ROW_TILE
    per_block = tok // ROW_TILE

    def wrap(value, size):
        return lax.rem(value + size, size)

    above, below = {"z": wrap(z + 1, nz)}, {"z": wrap(z - 1, nz)}

    def y_peer(d):
        return {"y": wrap(y + d, ny)}

    tp_peers = [(dx, dc) for dx in range(nx) for dc in range(nc) if dx or dc]

    def tp_peer(dx, dc):
        return {"x": wrap(x + dx, nx), "c": wrap(c + dc, nc)}

    def tp_from(dx, dc):
        return wrap(x - dx, nx) * nc + wrap(c - dc, nc)

    locals_ = [
        pltpu.make_async_copy(src, dst, local_sem.at[i])
        for i, (src, dst) in enumerate(
            [
                (k_hbm, kv_all.at[z, 0]),
                (v_hbm, kv_all.at[z, 1]),
                (gate_hbm, gate_all.at[z]),
                (q_hbm, q_all.at[y]),
                (up_hbm, up_all.at[z, y]),
                (dn_hbm, dn_all.at[z, y]),
                (res_hbm, res_all.at[tp]),
                (wo_hbm, wo_s),
            ]
        )
    ]
    for copy in locals_:
        copy.start()

    barrier = pltpu.get_barrier_semaphore()
    peers = [above, below] + [y_peer(d) for d in range(1, ny)]
    peers += [tp_peer(dx, dc) for dx, dc in tp_peers]
    for peer in peers:
        pl.semaphore_signal(barrier, inc=1, device_id=peer, device_id_type=MESH)
    pl.semaphore_wait(barrier, len(peers))

    def kv_copy(which, slot, up, step, device):
        ref = kv_all.at[slot, which]
        sems = ((kvu_sem, vu_sem) if up else (kvd_sem, vd_sem))[which]
        copies = (remote(ref, ref, sems.at[0, step - 1], sems.at[1, step - 1], device),)
        if which == 0:
            ref, sems = gate_all.at[slot], gu_sem if up else gd_sem
            copies += (remote(ref, ref, sems.at[0, step - 1], sems.at[1, step - 1], device),)
        return copies

    def kv_up_send(which, step):
        slot = z - step + 1
        return (slot >= 0) & (z < nz - 1), kv_copy(which, wrap(slot, nz), True, step, above)

    def kv_up_recv(which, step):
        return z - step >= 0, kv_copy(which, wrap(z - step, nz), True, step, above)

    def kv_down_send(which, step):
        slot = wrap(z + step - 1, nz)
        return slot < kv_down, kv_copy(which, slot, False, step, below)

    def kv_down_recv(which, step):
        slot = wrap(z + step, nz)
        return slot < kv_down, kv_copy(which, slot, False, step, below)

    def start(pair):
        when, copies = pair

        @pl.when(when)
        def _():
            for copy in copies:
                copy.start()

    def wait_recv(pair):
        when, copies = pair

        @pl.when(when)
        def _():
            for copy in copies:
                copy.wait_recv()

    def wait_send(pair):
        when, copies = pair

        @pl.when(when)
        def _():
            for copy in copies:
                copy.wait_send()

    def up_ring(sems, d, step, device, slot):
        ref = up_all.at[slot, wrap(y - d, ny), 0:FIRST_ROWS, :]
        return remote(ref, ref, sems.at[0, step - 1, d], sems.at[1, step - 1, d], device)

    def upu(d, step, arriving=False):
        return up_ring(upu_sem, d, step, above, wrap(z - step + (0 if arriving else 1), nz))

    def upd(d, step, arriving=False):
        return up_ring(upd_sem, d, step, below, wrap(z + step - (0 if arriving else 1), nz))

    def pass_upu(d, step):
        upu(d, step, True).wait_recv()
        if step < w_up:
            upu(d, step + 1).start()

    def pass_upd(d, step):
        upd(d, step, True).wait_recv()
        if step < w_down:
            upd(d, step + 1).start()

    def pass_dnu(step):
        for copy in dnu(step, True):
            copy.wait_recv()
        if step < w_up:
            start_all(dnu(step + 1))

    def pass_dnd(step):
        for copy in dnd(step, True):
            copy.wait_recv()
        if step < w_down:
            start_all(dnd(step + 1))

    def rest_ring(sems, rest_sems, step, device, slot):
        out = []
        for ref, s in ((dn_all.at[slot, y], sems), (up_all.at[slot, y, FIRST_ROWS:, :], rest_sems)):
            out.append(remote(ref, ref, s.at[0, step - 1], s.at[1, step - 1], device))
        return out

    def dnu(step, arriving=False):
        slot = wrap(z - step + (0 if arriving else 1), nz)
        return rest_ring(dnu_sem, u2u_sem, step, above, slot)

    def dnd(step, arriving=False):
        slot = wrap(z + step - (0 if arriving else 1), nz)
        return rest_ring(dnd_sem, u2d_sem, step, below, slot)

    def y_copies(buf_at, sems, arriving=False):
        out = []
        for d in range(1, ny):
            ref = buf_at(wrap(y - d, ny) if arriving else y)
            out.append(remote(ref, ref, sems.at[0, d - 1], sems.at[1, d - 1], y_peer(d)))
        return out

    rest_rows = slice(FIRST_ROWS, up_all.shape[2])

    def over_y(rest, k, side, arriving=False, half=False):
        buf, rows = (up_all, rest_rows) if rest else (dn_all, slice(0, dn_all.shape[2]))
        i = (1 - side) // 2
        source = y - side * ((1 if half else 0) + (1 if arriving else 0))
        if half:
            mid = (rows.start + rows.stop) // 2
            rows = slice(mid, rows.stop) if i else slice(rows.start, mid)
        ref = buf.at[wrap(z + k, nz), wrap(source, ny), rows, :]
        sems = (u2h_sem if rest else dnh_sem) if half else (u2y_sem if rest else dny_sem)
        sems = sems.at[k + w_up]
        return remote(ref, ref, sems.at[0, i], sems.at[1, i], y_peer(side))

    def send_y(rest, k):
        for side in (1, -1):
            over_y(rest, k, side).start()

    def pass_y(rest, k):
        for side in (1, -1):
            over_y(rest, k, side, True).wait_recv()
            over_y(rest, k, side, half=True).start()

    q_send = y_copies(lambda at: q_all.at[at], q_sem)
    q_arrive = y_copies(lambda at: q_all.at[at], q_sem, True)
    upy_send = y_copies(lambda at: up_all.at[z, at, 0:FIRST_ROWS, :], upy_sem)
    upy_arrive = y_copies(lambda at: up_all.at[z, at, 0:FIRST_ROWS, :], upy_sem, True)

    def tp_copies(buf, sems, arriving=False):
        out = []
        for i, (dx, dc) in enumerate(tp_peers):
            ref = buf.at[tp_from(dx, dc) if arriving else tp]
            out.append(remote(ref, ref, sems.at[0, i], sems.at[1, i], tp_peer(dx, dc)))
        return out

    res_send, res_arrive = tp_copies(res_all, res_sem), tp_copies(res_all, res_sem, True)

    def head_copy(d, arriving=False):
        ref = heads.at[wrap(x - d, nx) * nc + c if arriving else tp]
        return remote(ref, ref, head_sem.at[0, d - 1], head_sem.at[1, d - 1], {"x": wrap(x + d, nx)})

    def head_to_pair(d, arriving=False):
        ref = heads.at[wrap(x - d, nx) * nc + (1 - c if arriving else c)]
        return remote(ref, ref, pair_head_sem.at[0, d], pair_head_sem.at[1, d], {"c": 1 - c})

    def o_copies(arriving=False):
        out = []
        for d in range(1, ny):
            to = wrap(y + d, ny)
            source = wrap(y - d, ny) if arriving else y
            out.append(
                remote(o_send.at[to], o_recv.at[source], o_sem.at[0, d - 1], o_sem.at[1, d - 1], y_peer(d))
            )
            out.append(
                remote(
                    lse_send.at[to], lse_recv.at[source], lse_sem.at[0, d - 1], lse_sem.at[1, d - 1], y_peer(d)
                )
            )
        return out

    def start_all(copies):
        for copy in copies:
            copy.start()

    def move(kind, k, step=0):
        if kind == "ring":
            pass_dnd(k) if k > 0 else pass_dnu(-k)
        elif kind == "spread":
            send_y(step == 1, k)
        elif kind == "relay":
            pass_y(step == 1, k)
        elif kind == "down1":
            if k:
                upy_arrive[k - 1].wait_recv()
            upd(k, 1).start()
        elif kind == "up1":
            upu(k, 1).start()
        elif kind == "down":
            pass_upd(k, step)
        elif kind == "up":
            pass_upu(k, step)

    def at(place):
        for item in PLAN[place]:
            move(*item)

    locals_[0].wait()
    locals_[2].wait()
    start(kv_up_send(0, 1))
    start(kv_down_send(0, 1))
    locals_[1].wait()
    start(kv_up_send(1, 1))
    start(kv_down_send(1, 1))
    locals_[3].wait()
    start_all(q_send)
    locals_[4].wait()
    locals_[5].wait()
    start_all(dnd(1))
    start_all(dnu(1))
    start_all(upy_send)
    at(0)
    locals_[6].wait()
    start_all(res_send)

    top_s[...] = jnp.full_like(top_s, LOW)
    acc_s[...] = jnp.zeros_like(acc_s)
    v_ones[:, hd:] = jnp.ones((tok, hd), jnp.bfloat16)

    def attend(slot, first_tile, count, masked=False):
        for t in [first_tile + u for u in range(count)]:
            rows = pl.ds(t * ROW_TILE, ROW_TILE)
            q = q_all[t // per_block, pl.ds(lax.rem(t, per_block) * ROW_TILE, ROW_TILE), :]
            s = dot(q, kv_all[slot, 0], ((1,), (1,))) - gate_all[slot] * (hd**0.5)
            if masked:
                q_pos = t * ROW_TILE + lax.broadcasted_iota(jnp.int32, s.shape, 0)
                k_pos = y * tok + lax.broadcasted_iota(jnp.int32, s.shape, 1)
                s = jnp.where(k_pos <= q_pos, s, LOW)
            old = top_s[rows, :]
            new = jnp.maximum(old, jnp.max(s, axis=1, keepdims=True))
            fade = jnp.exp2((old - new) * to_exp2)
            weights = jnp.exp2((s - jnp.concatenate([new] * (tok // hd), axis=1)) * to_exp2)
            product = dot(weights.astype(jnp.bfloat16), v_ones[...])
            acc_s[rows, :] = acc_s[rows, :] * jnp.concatenate([fade, fade], axis=1) + product
            top_s[rows, :] = new

    v_ones[:, :hd] = kv_all[z, 1]
    attend(z, y * per_block, per_block, True)
    at(1)
    for copy in q_arrive:
        copy.wait_recv()

    def later_block(b, carry):
        attend(z, b * per_block, per_block)
        return carry

    lax.fori_loop(y + 1, ny, later_block, 0)

    def forward_kv(step):
        for which in range(2):
            wait_recv(kv_up_recv(which, step))
            if step < kv_up:
                start(kv_up_send(which, step + 1))
            if step <= kv_down:
                wait_recv(kv_down_recv(which, step))
                if step < kv_down:
                    start(kv_down_send(which, step + 1))

    def attend_step(step):
        first = jnp.where(z - step >= 0, 0, 1)
        last = jnp.where(z + step >= nz, 2, 1) if step <= kv_down else 1

        def block(u, carry):
            slot = wrap(z + (2 * u - 1) * step, nz)
            v_ones[:, :hd] = kv_all[slot, 1]
            attend(slot, 0, tiles)
            return carry

        lax.fori_loop(first, last, block, 0)

    at(2)
    for step in range(1, kv_up + 1):
        forward_kv(step)
        at(2 * step + 1)
        attend_step(step)
        at(2 * step + 2)

    eye = lax.broadcasted_iota(jnp.int32, (hd, hd), 0) == lax.broadcasted_iota(jnp.int32, (hd, hd), 1)

    for block in range(ny):
        for sub in range(tok // hd):
            rows = pl.ds(block * tok + sub * hd, hd)
            denom = jnp.maximum(acc_s[rows, hd:], 1e-30)
            o_send[block, sub * hd : (sub + 1) * hd, :] = (acc_s[rows, :hd] / denom).astype(jnp.bfloat16)
            lse = top_s[rows, :] * to_exp2 + jnp.log2(denom)
            line = jnp.sum(jnp.where(eye, lse, 0.0), axis=0, keepdims=True)
            lse_send[block, :, sub * hd : (sub + 1) * hd] = line
    start_all(o_copies())
    o_recv[y] = o_send[y]
    lse_recv[y] = lse_send[y]

    at(11)

    for copy in o_copies(True):
        copy.wait_recv()
    for sub in range(tok // hd):
        span = slice(sub * hd, (sub + 1) * hd)
        lines = [lse_recv[i, 0:1, span] for i in range(ny)]
        best = functools.reduce(jnp.maximum, lines)
        shares = [jnp.exp2(line - best) for line in lines]
        total = functools.reduce(jnp.add, shares)
        summed = jnp.zeros((hd, hd), jnp.float32)
        for i in range(ny):
            share = jnp.broadcast_to(shares[i] / total, (hd, hd))
            column = jnp.sum(jnp.where(eye, share, 0.0), axis=1, keepdims=True)
            summed = summed + column * o_recv[i, span, :].astype(jnp.float32)
        heads[tp, span, :] = summed.astype(jnp.bfloat16)
    for d in range(1, nx):
        head_copy(d).start()
    head_to_pair(0).start()

    at(12)

    locals_[7].wait()
    for copy in res_arrive:
        copy.wait_recv()
    for d in range(1, nx):
        head_copy(d, True).wait_recv()
        head_to_pair(d).start()
    at(13)
    for d in range(nx):
        head_to_pair(d, True).wait_recv()
    n_heads = heads.shape[0]

    def project(n, squares):
        cols = pl.ds(pl.multiple_of(n * COL_TILE, COL_TILE), COL_TILE)
        attended = jnp.concatenate([heads[h] for h in range(n_heads)], axis=1)
        base = res_all[:, :, cols].reshape(tok, COL_TILE).astype(jnp.float32)
        total = base + dot(attended, wo_s[:, cols])
        rsum[:, cols] = total
        return squares + jnp.sum(total * total, axis=1, keepdims=True)

    squares = jnp.zeros((tok, 1), jnp.float32)
    segment = width // COL_TILE // 4
    for i in range(4):
        squares = lax.fori_loop(i * segment, (i + 1) * segment, project, squares)
        at(14 + i)
    inverse = lax.rsqrt(squares / width + 1e-06)
    top_s[0:tok, :] = jnp.broadcast_to(inverse, (tok, hd))

    def normalise(r, carry):
        rows = pl.ds(pl.multiple_of(r * own_rows, own_rows), own_rows)
        factor = top_s[rows, 0:1]
        normed[rows, :] = (rsum[rows, :] * factor * gain_ref[...]).astype(jnp.bfloat16)
        return carry

    lax.fori_loop(0, tok // own_rows, normalise, 0)

    at(18)

    at(19)
    for k in range(-w_up, w_down + 1):
        for side in (1, -1):
            over_y(True, k, side, True, True).wait_recv()
    ff = hidden.shape[1]

    def up_tile(n, carry):
        cols = pl.ds(pl.multiple_of(n * COL_TILE, COL_TILE), COL_TILE)
        proj = dot(normed[...], up_all[:, :, :, cols].reshape(width, COL_TILE))
        hidden[:, cols] = jnp.square(jnp.maximum(proj, 0.0)).astype(jnp.bfloat16)
        return carry

    lax.fori_loop(0, ff // COL_TILE, up_tile, 0)

    z_cols = width // nz
    order = [0] + [s for k in range(1, w_up + 1) for s in (k, -k)] + list(range(w_up + 1, w_down + 1))

    def cols_of(k):
        return pl.ds(pl.multiple_of(wrap(z + k, nz) * z_cols, z_cols), z_cols)

    def pair_copy(k):
        return remote(
            part.at[1 - c, :, :, cols_of(k)],
            pair_recv.at[:, :, cols_of(k)],
            pair_sem.at[0, k + w_up],
            pair_sem.at[1, k + w_up],
            {"c": 1 - c},
        )

    def sum_copy(k, d):
        return remote(
            sum_send.at[d, :, cols_of(k)],
            sum_recv.at[d, :, cols_of(k)],
            sum_sem.at[0, k + w_up, d - 1],
            sum_sem.at[1, k + w_up, d - 1],
            {"x": wrap(x + d, nx)},
        )

    def finish_pair(k):
        cols = cols_of(k)
        pair_copy(k).wait_recv()
        for d in range(1, nx):
            at = wrap(x + d, nx)
            both = part[c, at, :, cols].astype(jnp.float32) + pair_recv[at, :, cols].astype(jnp.float32)
            sum_send[d, :, cols] = both.astype(jnp.bfloat16)
            sum_copy(k, d).start()

    for i, k in enumerate(order):
        at(20 + i)
        for side in (1, -1):
            over_y(False, k, side, True, True).wait_recv()
        block = dot(hidden[...], dn_all[wrap(z + k, nz)].reshape(z_cols, ff), ((1,), (1,)))
        for owner in range(nx * nc):
            part[owner % nc, owner // nc, :, cols_of(k)] = block[
                owner * own_rows : (owner + 1) * own_rows, :
            ].astype(jnp.bfloat16)
        pair_copy(k).start()
        if i:
            finish_pair(order[i - 1])
    finish_pair(order[-1])

    final = rsum[pl.ds(pl.multiple_of(tp * own_rows, own_rows), own_rows), :]
    final = final + (part[c, x].astype(jnp.float32) + pair_recv[x].astype(jnp.float32))
    for k in order:
        for d in range(1, nx):
            sum_copy(k, d).wait_recv()
    for d in range(1, nx):
        final = final + sum_recv[d].astype(jnp.float32)
    out_ref[...] = final.astype(jnp.bfloat16)

    for which in range(2):
        for step in range(1, kv_up + 1):
            wait_send(kv_up_send(which, step))
        for step in range(1, kv_down + 1):
            wait_send(kv_down_send(which, step))
    sent = q_send + upy_send + res_send + o_copies()
    sent += [head_copy(d) for d in range(1, nx)] + [head_to_pair(d) for d in range(nx)]
    for step in range(1, w_up + 1):
        sent += dnu(step) + [upu(d, step) for d in range(ny)]
    for step in range(1, w_down + 1):
        sent += dnd(step) + [upd(d, step) for d in range(ny)]
    for k in order:
        for rest in (True, False):
            for side in (1, -1):
                sent += [over_y(rest, k, side), over_y(rest, k, side, half=True)]
        sent += [pair_copy(k)] + [sum_copy(k, d) for d in range(1, nx)]
    for copy in sent:
        copy.wait_send()


def per_device(sizes, queries, keys, values, cum_gate, residual, w_out, gain, w_up, w_down):
    nz, ny, nx, nc = sizes
    ntp = nx * nc
    tok, hd = queries.shape
    rows, width = residual.shape
    depth, ff = w_up.shape
    gates = cum_gate.reshape(1, tok)
    bf16, f32 = jnp.bfloat16, jnp.float32
    anywhere = pl.BlockSpec(memory_space=pl.ANY)
    in_vmem = pl.BlockSpec(memory_space=pltpu.VMEM)
    dma = pltpu.SemaphoreType.DMA
    up_steps, down_steps = nz // 2, nz - 1 - nz // 2
    return pl.pallas_call(
        functools.partial(layer_kernel, sizes),
        out_shape=jax.ShapeDtypeStruct((rows, width), bf16),
        in_specs=[anywhere] * 6 + [in_vmem] + [anywhere] * 2,
        out_specs=in_vmem,
        scratch_shapes=[
            pltpu.VMEM((ny, tok, hd), bf16),
            pltpu.VMEM((nz, 2, tok, hd), bf16),
            pltpu.VMEM((nz, 1, tok), f32),
            pltpu.VMEM((tok, 2 * hd), bf16),
            pltpu.VMEM((ny * tok, hd), f32),
            pltpu.VMEM((ny * tok, 2 * hd), f32),
            pltpu.VMEM((ny, tok, hd), bf16),
            pltpu.VMEM((ny, tok, hd), bf16),
            pltpu.VMEM((ny, 1, tok), f32),
            pltpu.VMEM((ny, 1, tok), f32),
            pltpu.VMEM((ntp, tok, hd), bf16),
            pltpu.VMEM((ntp, rows, width), bf16),
            pltpu.VMEM(w_out.shape, bf16),
            pltpu.VMEM((tok, width), f32),
            pltpu.VMEM((tok, width), bf16),
            pltpu.VMEM((nz, ny, depth, ff), bf16),
            pltpu.VMEM((nz, ny, depth, ff), bf16),
            pltpu.VMEM((tok, ff), bf16),
            pltpu.VMEM((nc, nx, rows, width), bf16),
            pltpu.VMEM((nx, rows, width), bf16),
            pltpu.VMEM((nx, rows, width), bf16),
            pltpu.VMEM((nx, rows, width), bf16),
            dma((8,)),
            dma((2, ny - 1)),
            dma((2, up_steps)),
            dma((2, down_steps)),
            dma((2, up_steps)),
            dma((2, down_steps)),
            dma((2, up_steps)),
            dma((2, down_steps)),
            dma((2, ny - 1)),
            dma((2, ny - 1)),
            dma((2, nx - 1)),
            dma((2, nx)),
            dma((2, ntp - 1)),
            dma((2, ny - 1)),
            dma((2, down_steps, ny)),
            dma((2, up_steps, ny)),
            dma((2, down_steps)),
            dma((2, up_steps)),
            dma((nz, 2, 2)),
            dma((nz, 2, 2)),
            dma((2, down_steps)),
            dma((2, up_steps)),
            dma((nz, 2, 2)),
            dma((nz, 2, 2)),
            dma((2, nz)),
            dma((2, nz, nx - 1)),
        ],
        compiler_params=pltpu.CompilerParams(
            collective_id=0, has_side_effects=True, vmem_limit_bytes=63 * 1024 * 1024
        ),
    )(queries, keys, values, gates, residual, w_out, gain.reshape(1, width), w_up, w_down.T)


def solution(mesh):
    finer = Mesh(mesh.devices.reshape(GRID), ("z", "y", "x", "c"))
    sp, tp = ("z", "y"), ("x", "c")
    rows = ("z", "y", "x", "c")
    in_specs = (
        P(sp, tp),
        P(sp, tp),
        P(sp, tp),
        P(sp, tp),
        P(rows, None),
        P(),
        P(),
        P(sp, tp),
        P(tp, sp),
    )
    return jax.shard_map(
        functools.partial(per_device, GRID),
        mesh=finer,
        in_specs=in_specs,
        out_specs=P(rows, None),
        check_vma=False,
    )
```

```python
import functools
import math

import jax
import jax.numpy as jnp
from jax import lax
from jax.experimental import pallas as pl
from jax.experimental.pallas import tpu as pltpu
from jax.sharding import Mesh
from jax.sharding import PartitionSpec as P

MESH = pl.DeviceIdType.MESH
GRID = (8, 4, 4, 2)
ROW_TILE = 256
COL_TILE = 256
FIRST_ROWS = 32
LOW = -1e30

PLAN = {
    0: [],
    1: [("spread", 0, 1), ("down1", 0)],
    2: [],
    3: [("down1", 1)],
    4: [("ring", 1), ("ring", -1), ("spread", 0, 0), ("spread", 1, 0), ("spread", -1, 1), ("ring", -2), ("spread", -2, 0), ("spread", -1, 0)],
    5: [("down", 0, 1), ("down1", 2), ("relay", 0, 0), ("spread", 1, 1), ("relay", 1, 0)],
    6: [("ring", 2), ("up1", 1), ("spread", 2, 0), ("down", 2, 1), ("spread", -2, 1)],
    7: [("relay", -1, 1), ("spread", 2, 1), ("up", 1, 1)],
    8: [],
    9: [("relay", 0, 1), ("down", 1, 1), ("ring", 3), ("down1", 3), ("up1", 3)],
    10: [("down", 0, 2), ("up", 1, 2)],
    11: [("up1", 2), ("relay", 2, 1), ("down", 3, 1), ("up", 3, 1), ("ring", -3), ("ring", 4), ("spread", 3, 1), ("up1", 0), ("down", 2, 2), ("spread", -3, 1), ("relay", -2, 1)],
    12: [("spread", 4, 1), ("down", 3, 2), ("relay", 3, 1), ("up", 0, 1), ("down", 0, 3), ("spread", 3, 0), ("up", 3, 2), ("down", 1, 2), ("up", 2, 1), ("up", 0, 2)],
    13: [("relay", 4, 1), ("relay", 1, 1), ("relay", -3, 1), ("down", 2, 3), ("down", 1, 3), ("down", 3, 3), ("relay", -1, 0), ("down", 0, 4)],
    14: [],
    15: [("up", 2, 2), ("spread", -3, 0), ("up", 1, 3), ("relay", 3, 0)],
    16: [("relay", -2, 0), ("down", 2, 4)],
    17: [],
    18: [("relay", 2, 0)],
    19: [("down", 3, 4), ("up", 2, 3), ("up", 3, 3), ("up", 0, 3), ("down", 1, 4)],
    20: [("spread", 4, 0)],
    21: [],
    22: [],
    23: [("relay", -3, 0)],
    24: [],
    25: [("relay", 4, 0)],
    26: [],
    27: [],
}


def remote(src, dst, send_sem, recv_sem, device):
    return pltpu.make_async_remote_copy(
        src_ref=src,
        dst_ref=dst,
        send_sem=send_sem,
        recv_sem=recv_sem,
        device_id=device,
        device_id_type=MESH,
    )


def dot(a, b, contract=((1,), (0,))):
    return lax.dot_general(a, b, (contract, ((), ())), preferred_element_type=jnp.float32)


def layer_kernel(
    sizes,
    q_hbm,
    k_hbm,
    v_hbm,
    gate_hbm,
    res_hbm,
    wo_hbm,
    gain_ref,
    up_hbm,
    dn_hbm,
    out_ref,
    q_all,
    kv_all,
    gate_all,
    v_ones,
    top_s,
    acc_s,
    o_send,
    o_recv,
    lse_send,
    lse_recv,
    heads,
    res_all,
    wo_s,
    rsum,
    normed,
    up_all,
    dn_all,
    hidden,
    part,
    pair_recv,
    sum_send,
    sum_recv,
    local_sem,
    q_sem,
    kvu_sem,
    kvd_sem,
    gu_sem,
    gd_sem,
    vu_sem,
    vd_sem,
    o_sem,
    lse_sem,
    head_sem,
    pair_head_sem,
    res_sem,
    upy_sem,
    upu_sem,
    upd_sem,
    dnu_sem,
    dnd_sem,
    dny_sem,
    dnh_sem,
    u2u_sem,
    u2d_sem,
    u2y_sem,
    u2h_sem,
    pair_sem,
    sum_sem,
):
    nz, ny, nx, nc = sizes
    z, y, x, c = (lax.axis_index(name) for name in ("z", "y", "x", "c"))
    tp = x * nc + c
    tok, hd = q_all.shape[1], q_all.shape[2]
    own_rows, width = out_ref.shape
    to_exp2 = hd**-0.5 * math.log2(math.e)
    kv_up, kv_down = nz // 2, nz - 1 - nz // 2
    w_up, w_down = nz - 1 - nz // 2, nz // 2
    tiles = ny * tok // ROW_TILE
    per_block = tok // ROW_TILE

    def wrap(value, size):
        return lax.rem(value + size, size)

    above, below = {"z": wrap(z + 1, nz)}, {"z": wrap(z - 1, nz)}

    def y_peer(d):
        return {"y": wrap(y + d, ny)}

    tp_peers = [(dx, dc) for dx in range(nx) for dc in range(nc) if dx or dc]

    def tp_peer(dx, dc):
        return {"x": wrap(x + dx, nx), "c": wrap(c + dc, nc)}

    def tp_from(dx, dc):
        return wrap(x - dx, nx) * nc + wrap(c - dc, nc)

    locals_ = [
        pltpu.make_async_copy(src, dst, local_sem.at[i])
        for i, (src, dst) in enumerate(
            [
                (k_hbm, kv_all.at[z, 0]),
                (v_hbm, kv_all.at[z, 1]),
                (gate_hbm, gate_all.at[z]),
                (q_hbm, q_all.at[y]),
                (up_hbm, up_all.at[z, y]),
                (dn_hbm, dn_all.at[z, y]),
                (res_hbm, res_all.at[tp]),
                (wo_hbm, wo_s),
            ]
        )
    ]
    for copy in locals_:
        copy.start()

    barrier = pltpu.get_barrier_semaphore()
    peers = [above, below] + [y_peer(d) for d in range(1, ny)]
    peers += [tp_peer(dx, dc) for dx, dc in tp_peers]
    for peer in peers:
        pl.semaphore_signal(barrier, inc=1, device_id=peer, device_id_type=MESH)
    pl.semaphore_wait(barrier, len(peers))

    def kv_copy(which, slot, up, step, device):
        ref = kv_all.at[slot, which]
        sems = ((kvu_sem, vu_sem) if up else (kvd_sem, vd_sem))[which]
        copies = (remote(ref, ref, sems.at[0, step - 1], sems.at[1, step - 1], device),)
        if which == 0:
            ref, sems = gate_all.at[slot], gu_sem if up else gd_sem
            copies += (remote(ref, ref, sems.at[0, step - 1], sems.at[1, step - 1], device),)
        return copies

    def kv_up_send(which, step):
        slot = z - step + 1
        return (slot >= 0) & (z < nz - 1), kv_copy(which, wrap(slot, nz), True, step, above)

    def kv_up_recv(which, step):
        return z - step >= 0, kv_copy(which, wrap(z - step, nz), True, step, above)

    def kv_down_send(which, step):
        slot = wrap(z + step - 1, nz)
        return slot < kv_down, kv_copy(which, slot, False, step, below)

    def kv_down_recv(which, step):
        slot = wrap(z + step, nz)
        return slot < kv_down, kv_copy(which, slot, False, step, below)

    def start(pair):
        when, copies = pair

        @pl.when(when)
        def _():
            for copy in copies:
                copy.start()

    def wait_recv(pair):
        when, copies = pair

        @pl.when(when)
        def _():
            for copy in copies:
                copy.wait_recv()

    def wait_send(pair):
        when, copies = pair

        @pl.when(when)
        def _():
            for copy in copies:
                copy.wait_send()

    def up_ring(sems, d, step, device, slot):
        ref = up_all.at[slot, wrap(y - d, ny), 0:FIRST_ROWS, :]
        return remote(ref, ref, sems.at[0, step - 1, d], sems.at[1, step - 1, d], device)

    def upu(d, step, arriving=False):
        return up_ring(upu_sem, d, step, above, wrap(z - step + (0 if arriving else 1), nz))

    def upd(d, step, arriving=False):
        return up_ring(upd_sem, d, step, below, wrap(z + step - (0 if arriving else 1), nz))

    def pass_upu(d, step):
        upu(d, step, True).wait_recv()
        if step < w_up:
            upu(d, step + 1).start()

    def pass_upd(d, step):
        upd(d, step, True).wait_recv()
        if step < w_down:
            upd(d, step + 1).start()

    def pass_dnu(step):
        for copy in dnu(step, True):
            copy.wait_recv()
        if step < w_up:
            start_all(dnu(step + 1))

    def pass_dnd(step):
        for copy in dnd(step, True):
            copy.wait_recv()
        if step < w_down:
            start_all(dnd(step + 1))

    def rest_ring(sems, rest_sems, step, device, slot):
        out = []
        for ref, s in ((dn_all.at[slot, y], sems), (up_all.at[slot, y, FIRST_ROWS:, :], rest_sems)):
            out.append(remote(ref, ref, s.at[0, step - 1], s.at[1, step - 1], device))
        return out

    def dnu(step, arriving=False):
        slot = wrap(z - step + (0 if arriving else 1), nz)
        return rest_ring(dnu_sem, u2u_sem, step, above, slot)

    def dnd(step, arriving=False):
        slot = wrap(z + step - (0 if arriving else 1), nz)
        return rest_ring(dnd_sem, u2d_sem, step, below, slot)

    def y_copies(buf_at, sems, arriving=False):
        out = []
        for d in range(1, ny):
            ref = buf_at(wrap(y - d, ny) if arriving else y)
            out.append(remote(ref, ref, sems.at[0, d - 1], sems.at[1, d - 1], y_peer(d)))
        return out

    rest_rows = slice(FIRST_ROWS, up_all.shape[2])

    def over_y(rest, k, side, arriving=False, half=False):
        buf, rows = (up_all, rest_rows) if rest else (dn_all, slice(0, dn_all.shape[2]))
        i = (1 - side) // 2
        source = y - side * ((1 if half else 0) + (1 if arriving else 0))
        if half:
            mid = (rows.start + rows.stop) // 2
            rows = slice(mid, rows.stop) if i else slice(rows.start, mid)
        ref = buf.at[wrap(z + k, nz), wrap(source, ny), rows, :]
        sems = (u2h_sem if rest else dnh_sem) if half else (u2y_sem if rest else dny_sem)
        sems = sems.at[k + w_up]
        return remote(ref, ref, sems.at[0, i], sems.at[1, i], y_peer(side))

    def send_y(rest, k):
        for side in (1, -1):
            over_y(rest, k, side).start()

    def pass_y(rest, k):
        for side in (1, -1):
            over_y(rest, k, side, True).wait_recv()
            over_y(rest, k, side, half=True).start()

    q_send = y_copies(lambda at: q_all.at[at], q_sem)
    q_arrive = y_copies(lambda at: q_all.at[at], q_sem, True)
    upy_send = y_copies(lambda at: up_all.at[z, at, 0:FIRST_ROWS, :], upy_sem)
    upy_arrive = y_copies(lambda at: up_all.at[z, at, 0:FIRST_ROWS, :], upy_sem, True)

    def tp_copies(buf, sems, arriving=False):
        out = []
        for i, (dx, dc) in enumerate(tp_peers):
            ref = buf.at[tp_from(dx, dc) if arriving else tp]
            out.append(remote(ref, ref, sems.at[0, i], sems.at[1, i], tp_peer(dx, dc)))
        return out

    res_send, res_arrive = tp_copies(res_all, res_sem), tp_copies(res_all, res_sem, True)

    def head_copy(d, arriving=False):
        ref = heads.at[wrap(x - d, nx) * nc + c if arriving else tp]
        return remote(ref, ref, head_sem.at[0, d - 1], head_sem.at[1, d - 1], {"x": wrap(x + d, nx)})

    def head_to_pair(d, arriving=False):
        ref = heads.at[wrap(x - d, nx) * nc + (1 - c if arriving else c)]
        return remote(ref, ref, pair_head_sem.at[0, d], pair_head_sem.at[1, d], {"c": 1 - c})

    def o_copies(arriving=False):
        out = []
        for d in range(1, ny):
            to = wrap(y + d, ny)
            source = wrap(y - d, ny) if arriving else y
            out.append(
                remote(o_send.at[to], o_recv.at[source], o_sem.at[0, d - 1], o_sem.at[1, d - 1], y_peer(d))
            )
            out.append(
                remote(
                    lse_send.at[to], lse_recv.at[source], lse_sem.at[0, d - 1], lse_sem.at[1, d - 1], y_peer(d)
                )
            )
        return out

    def start_all(copies):
        for copy in copies:
            copy.start()

    def move(kind, k, step=0):
        if kind == "ring":
            pass_dnd(k) if k > 0 else pass_dnu(-k)
        elif kind == "spread":
            send_y(step == 1, k)
        elif kind == "relay":
            pass_y(step == 1, k)
        elif kind == "down1":
            if k:
                upy_arrive[k - 1].wait_recv()
            upd(k, 1).start()
        elif kind == "up1":
            upu(k, 1).start()
        elif kind == "down":
            pass_upd(k, step)
        elif kind == "up":
            pass_upu(k, step)

    def at(place):
        for item in PLAN[place]:
            move(*item)

    locals_[0].wait()
    locals_[2].wait()
    start(kv_up_send(0, 1))
    start(kv_down_send(0, 1))
    locals_[1].wait()
    start(kv_up_send(1, 1))
    start(kv_down_send(1, 1))
    locals_[3].wait()
    start_all(q_send)
    locals_[4].wait()
    locals_[5].wait()
    start_all(dnd(1))
    start_all(dnu(1))
    start_all(upy_send)
    at(0)
    locals_[6].wait()
    start_all(res_send)

    top_s[...] = jnp.full_like(top_s, LOW)
    acc_s[...] = jnp.zeros_like(acc_s)
    v_ones[:, hd:] = jnp.ones((tok, hd), jnp.bfloat16)

    def attend(slot, first_tile, count, masked=False):
        for t in [first_tile + u for u in range(count)]:
            rows = pl.ds(t * ROW_TILE, ROW_TILE)
            q = q_all[t // per_block, pl.ds(lax.rem(t, per_block) * ROW_TILE, ROW_TILE), :]
            s = dot(q, kv_all[slot, 0], ((1,), (1,))) - gate_all[slot] * (hd**0.5)
            if masked:
                q_pos = t * ROW_TILE + lax.broadcasted_iota(jnp.int32, s.shape, 0)
                k_pos = y * tok + lax.broadcasted_iota(jnp.int32, s.shape, 1)
                s = jnp.where(k_pos <= q_pos, s, LOW)
            old = top_s[rows, :]
            new = jnp.maximum(old, jnp.max(s, axis=1, keepdims=True))
            fade = jnp.exp2((old - new) * to_exp2)
            weights = jnp.exp2((s - jnp.concatenate([new] * (tok // hd), axis=1)) * to_exp2)
            product = dot(weights.astype(jnp.bfloat16), v_ones[...])
            acc_s[rows, :] = acc_s[rows, :] * jnp.concatenate([fade, fade], axis=1) + product
            top_s[rows, :] = new

    v_ones[:, :hd] = kv_all[z, 1]
    attend(z, y * per_block, per_block, True)
    at(1)
    for copy in q_arrive:
        copy.wait_recv()

    def later_block(b, carry):
        attend(z, b * per_block, per_block)
        return carry

    lax.fori_loop(y + 1, ny, later_block, 0)

    def forward_kv(step):
        for which in range(2):
            wait_recv(kv_up_recv(which, step))
            if step < kv_up:
                start(kv_up_send(which, step + 1))
            if step <= kv_down:
                wait_recv(kv_down_recv(which, step))
                if step < kv_down:
                    start(kv_down_send(which, step + 1))

    def attend_step(step):
        first = jnp.where(z - step >= 0, 0, 1)
        last = jnp.where(z + step >= nz, 2, 1) if step <= kv_down else 1

        def block(u, carry):
            slot = wrap(z + (2 * u - 1) * step, nz)
            v_ones[:, :hd] = kv_all[slot, 1]
            attend(slot, 0, tiles)
            return carry

        lax.fori_loop(first, last, block, 0)

    at(2)
    for step in range(1, kv_up + 1):
        forward_kv(step)
        at(2 * step + 1)
        attend_step(step)
        at(2 * step + 2)

    eye = lax.broadcasted_iota(jnp.int32, (hd, hd), 0) == lax.broadcasted_iota(jnp.int32, (hd, hd), 1)

    for block in range(ny):
        for sub in range(tok // hd):
            rows = pl.ds(block * tok + sub * hd, hd)
            denom = jnp.maximum(acc_s[rows, hd:], 1e-30)
            o_send[block, sub * hd : (sub + 1) * hd, :] = (acc_s[rows, :hd] / denom).astype(jnp.bfloat16)
            lse = top_s[rows, :] * to_exp2 + jnp.log2(denom)
            line = jnp.sum(jnp.where(eye, lse, 0.0), axis=0, keepdims=True)
            lse_send[block, :, sub * hd : (sub + 1) * hd] = line
    start_all(o_copies())
    o_recv[y] = o_send[y]
    lse_recv[y] = lse_send[y]

    at(11)

    for copy in o_copies(True):
        copy.wait_recv()
    for sub in range(tok // hd):
        span = slice(sub * hd, (sub + 1) * hd)
        lines = [lse_recv[i, 0:1, span] for i in range(ny)]
        best = functools.reduce(jnp.maximum, lines)
        shares = [jnp.exp2(line - best) for line in lines]
        total = functools.reduce(jnp.add, shares)
        summed = jnp.zeros((hd, hd), jnp.float32)
        for i in range(ny):
            share = jnp.broadcast_to(shares[i] / total, (hd, hd))
            column = jnp.sum(jnp.where(eye, share, 0.0), axis=1, keepdims=True)
            summed = summed + column * o_recv[i, span, :].astype(jnp.float32)
        heads[tp, span, :] = summed.astype(jnp.bfloat16)
    for d in range(1, nx):
        head_copy(d).start()
    head_to_pair(0).start()

    at(12)

    locals_[7].wait()
    for copy in res_arrive:
        copy.wait_recv()
    for d in range(1, nx):
        head_copy(d, True).wait_recv()
        head_to_pair(d).start()
    at(13)
    for d in range(nx):
        head_to_pair(d, True).wait_recv()
    n_heads = heads.shape[0]

    def project(n, squares):
        cols = pl.ds(pl.multiple_of(n * COL_TILE, COL_TILE), COL_TILE)
        attended = jnp.concatenate([heads[h] for h in range(n_heads)], axis=1)
        base = res_all[:, :, cols].reshape(tok, COL_TILE).astype(jnp.float32)
        total = base + dot(attended, wo_s[:, cols])
        rsum[:, cols] = total
        return squares + jnp.sum(total * total, axis=1, keepdims=True)

    squares = jnp.zeros((tok, 1), jnp.float32)
    segment = width // COL_TILE // 4
    for i in range(4):
        squares = lax.fori_loop(i * segment, (i + 1) * segment, project, squares)
        at(14 + i)
    inverse = lax.rsqrt(squares / width + 1e-06)
    top_s[0:tok, :] = jnp.broadcast_to(inverse, (tok, hd))

    def normalise(r, carry):
        rows = pl.ds(pl.multiple_of(r * own_rows, own_rows), own_rows)
        factor = top_s[rows, 0:1]
        normed[rows, :] = (rsum[rows, :] * factor * gain_ref[...]).astype(jnp.bfloat16)
        return carry

    lax.fori_loop(0, tok // own_rows, normalise, 0)

    at(18)

    z_cols = width // nz
    ff = hidden.shape[1]
    far = [-w_up, w_down]
    near = [k for k in range(-w_up, w_down + 1) if k not in far]

    def rest_arrived(levels):
        for k in levels:
            for side in (1, -1):
                over_y(True, k, side, True, True).wait_recv()

    def up_part(levels, cols):
        total = None
        for k in levels:
            slot = wrap(z + k, nz)
            rows = pl.ds(pl.multiple_of(slot * z_cols, z_cols), z_cols)
            term = dot(normed[:, rows], up_all[slot, :, :, cols].reshape(z_cols, COL_TILE))
            total = term if total is None else total + term
        return total

    def near_tile(n, carry):
        cols = pl.ds(pl.multiple_of(n * COL_TILE, COL_TILE), COL_TILE)
        acc_s[pl.ds(pl.multiple_of(n * tok, tok), tok), :] = up_part(near, cols)
        return carry

    def far_tile(n, carry):
        cols = pl.ds(pl.multiple_of(n * COL_TILE, COL_TILE), COL_TILE)
        proj = acc_s[pl.ds(pl.multiple_of(n * tok, tok), tok), :] + up_part(far, cols)
        hidden[:, cols] = jnp.square(jnp.maximum(proj, 0.0)).astype(jnp.bfloat16)
        return carry

    rest_arrived(near)
    lax.fori_loop(0, ff // COL_TILE, near_tile, 0)
    at(19)
    rest_arrived(far)
    lax.fori_loop(0, ff // COL_TILE, far_tile, 0)

    order = [0] + [s for k in range(1, w_up + 1) for s in (k, -k)] + list(range(w_up + 1, w_down + 1))

    def cols_of(k):
        return pl.ds(pl.multiple_of(wrap(z + k, nz) * z_cols, z_cols), z_cols)

    def pair_copy(k):
        return remote(
            part.at[1 - c, :, :, cols_of(k)],
            pair_recv.at[:, :, cols_of(k)],
            pair_sem.at[0, k + w_up],
            pair_sem.at[1, k + w_up],
            {"c": 1 - c},
        )

    def sum_copy(k, d):
        return remote(
            sum_send.at[d, :, cols_of(k)],
            sum_recv.at[d, :, cols_of(k)],
            sum_sem.at[0, k + w_up, d - 1],
            sum_sem.at[1, k + w_up, d - 1],
            {"x": wrap(x + d, nx)},
        )

    def finish_pair(k):
        cols = cols_of(k)
        pair_copy(k).wait_recv()
        for d in range(1, nx):
            at = wrap(x + d, nx)
            both = part[c, at, :, cols].astype(jnp.float32) + pair_recv[at, :, cols].astype(jnp.float32)
            sum_send[d, :, cols] = both.astype(jnp.bfloat16)
            sum_copy(k, d).start()

    for i, k in enumerate(order):
        at(20 + i)
        for side in (1, -1):
            over_y(False, k, side, True, True).wait_recv()
        block = dot(hidden[...], dn_all[wrap(z + k, nz)].reshape(z_cols, ff), ((1,), (1,)))
        for owner in range(nx * nc):
            part[owner % nc, owner // nc, :, cols_of(k)] = block[
                owner * own_rows : (owner + 1) * own_rows, :
            ].astype(jnp.bfloat16)
        pair_copy(k).start()
        if i:
            finish_pair(order[i - 1])
    finish_pair(order[-1])

    final = rsum[pl.ds(pl.multiple_of(tp * own_rows, own_rows), own_rows), :]
    final = final + (part[c, x].astype(jnp.float32) + pair_recv[x].astype(jnp.float32))
    for k in order:
        for d in range(1, nx):
            sum_copy(k, d).wait_recv()
    for d in range(1, nx):
        final = final + sum_recv[d].astype(jnp.float32)
    out_ref[...] = final.astype(jnp.bfloat16)

    for which in range(2):
        for step in range(1, kv_up + 1):
            wait_send(kv_up_send(which, step))
        for step in range(1, kv_down + 1):
            wait_send(kv_down_send(which, step))
    sent = q_send + upy_send + res_send + o_copies()
    sent += [head_copy(d) for d in range(1, nx)] + [head_to_pair(d) for d in range(nx)]
    for step in range(1, w_up + 1):
        sent += dnu(step) + [upu(d, step) for d in range(ny)]
    for step in range(1, w_down + 1):
        sent += dnd(step) + [upd(d, step) for d in range(ny)]
    for k in order:
        for rest in (True, False):
            for side in (1, -1):
                sent += [over_y(rest, k, side), over_y(rest, k, side, half=True)]
        sent += [pair_copy(k)] + [sum_copy(k, d) for d in range(1, nx)]
    for copy in sent:
        copy.wait_send()


def per_device(sizes, queries, keys, values, cum_gate, residual, w_out, gain, w_up, w_down):
    nz, ny, nx, nc = sizes
    ntp = nx * nc
    tok, hd = queries.shape
    rows, width = residual.shape
    depth, ff = w_up.shape
    gates = cum_gate.reshape(1, tok)
    bf16, f32 = jnp.bfloat16, jnp.float32
    anywhere = pl.BlockSpec(memory_space=pl.ANY)
    in_vmem = pl.BlockSpec(memory_space=pltpu.VMEM)
    dma = pltpu.SemaphoreType.DMA
    up_steps, down_steps = nz // 2, nz - 1 - nz // 2
    return pl.pallas_call(
        functools.partial(layer_kernel, sizes),
        out_shape=jax.ShapeDtypeStruct((rows, width), bf16),
        in_specs=[anywhere] * 6 + [in_vmem] + [anywhere] * 2,
        out_specs=in_vmem,
        scratch_shapes=[
            pltpu.VMEM((ny, tok, hd), bf16),
            pltpu.VMEM((nz, 2, tok, hd), bf16),
            pltpu.VMEM((nz, 1, tok), f32),
            pltpu.VMEM((tok, 2 * hd), bf16),
            pltpu.VMEM((ny * tok, hd), f32),
            pltpu.VMEM((ny * tok, 2 * hd), f32),
            pltpu.VMEM((ny, tok, hd), bf16),
            pltpu.VMEM((ny, tok, hd), bf16),
            pltpu.VMEM((ny, 1, tok), f32),
            pltpu.VMEM((ny, 1, tok), f32),
            pltpu.VMEM((ntp, tok, hd), bf16),
            pltpu.VMEM((ntp, rows, width), bf16),
            pltpu.VMEM(w_out.shape, bf16),
            pltpu.VMEM((tok, width), f32),
            pltpu.VMEM((tok, width), bf16),
            pltpu.VMEM((nz, ny, depth, ff), bf16),
            pltpu.VMEM((nz, ny, depth, ff), bf16),
            pltpu.VMEM((tok, ff), bf16),
            pltpu.VMEM((nc, nx, rows, width), bf16),
            pltpu.VMEM((nx, rows, width), bf16),
            pltpu.VMEM((nx, rows, width), bf16),
            pltpu.VMEM((nx, rows, width), bf16),
            dma((8,)),
            dma((2, ny - 1)),
            dma((2, up_steps)),
            dma((2, down_steps)),
            dma((2, up_steps)),
            dma((2, down_steps)),
            dma((2, up_steps)),
            dma((2, down_steps)),
            dma((2, ny - 1)),
            dma((2, ny - 1)),
            dma((2, nx - 1)),
            dma((2, nx)),
            dma((2, ntp - 1)),
            dma((2, ny - 1)),
            dma((2, down_steps, ny)),
            dma((2, up_steps, ny)),
            dma((2, down_steps)),
            dma((2, up_steps)),
            dma((nz, 2, 2)),
            dma((nz, 2, 2)),
            dma((2, down_steps)),
            dma((2, up_steps)),
            dma((nz, 2, 2)),
            dma((nz, 2, 2)),
            dma((2, nz)),
            dma((2, nz, nx - 1)),
        ],
        compiler_params=pltpu.CompilerParams(
            collective_id=0, has_side_effects=True, vmem_limit_bytes=63 * 1024 * 1024
        ),
    )(queries, keys, values, gates, residual, w_out, gain.reshape(1, width), w_up, w_down.T)


def solution(mesh):
    finer = Mesh(mesh.devices.reshape(GRID), ("z", "y", "x", "c"))
    sp, tp = ("z", "y"), ("x", "c")
    rows = ("z", "y", "x", "c")
    in_specs = (
        P(sp, tp),
        P(sp, tp),
        P(sp, tp),
        P(sp, tp),
        P(rows, None),
        P(),
        P(),
        P(sp, tp),
        P(tp, sp),
    )
    return jax.shard_map(
        functools.partial(per_device, GRID),
        mesh=finer,
        in_specs=in_specs,
        out_specs=P(rows, None),
        check_vma=False,
    )
```
